128 devices in a mesh: sp: 16 (over z, x), tp: 8 (over y, core).
Axes of the slice: x: 4, y: 4, z: 4, core: 2. Of those that a mesh axis runs over, the one named last changes fastest.
Arguments:
- queries: bfloat16 [16384, 512], P('sp', 'tp'), may hold values from -16 to 16
- key_heads: bfloat16 [16384, 512], P('sp', 'tp'), may hold values from -16 to 16
- value_heads: bfloat16 [16384, 512], P('sp', 'tp'), may hold values from -6 to 6
- head_gain: float32 [512], P('tp'), may hold values from 0.1 to 1.9
- residual: bfloat16 [16384, 2048], P(('sp', 'tp')), may hold values from -6 to 6
- out_weight: bfloat16 [512, 2048], replicated, may hold values from -0.25 to 0.25
- norm_gain: float32 [2048], replicated, may hold values from 0.1 to 1.9
- shared_gate: bfloat16 [2048, 512], replicated, may hold values from -0.125 to 0.125
- shared_up: bfloat16 [2048, 512], replicated, may hold values from -0.125 to 0.125
- shared_down: bfloat16 [512, 2048], replicated, may hold values from -0.25 to 0.25
- expert_gate: bfloat16 [256, 2048, 512], P(('sp', 'tp')), may hold values from -0.125 to 0.125
- expert_up: bfloat16 [256, 2048, 512], P(('sp', 'tp')), may hold values from -0.125 to 0.125
- expert_down: bfloat16 [256, 512, 2048], P(('sp', 'tp')), may hold values from -0.25 to 0.25
- routed_experts: int32 [16384, 4], P(('sp', 'tp')), may hold values from 0 to 255, all different within a row; in each aligned block of 128 rows (0 to 127, 128 to 255, ...) at most 3 rows name the same one
- route_weights: float32 [16384, 4], P(('sp', 'tp')), may hold values from 0.1 to 1.5
Outputs:
- layer_output: bfloat16 [16384, 2048], P(('sp', 'tp'))
The draws below stay inside these ranges and needn't reach their ends.
Inputs may be any that keep to these rules, and one draw needn't show every extreme that they name: `routed_experts`: each row names 4 different experts. Within the rows of one device (128 consecutive rows, aligned) no expert is named more than 3 times, and in every draw some expert is named exactly 3 times in some device's rows.
All inputs are finite; a program needn't handle non-finite values.
Results may differ from the reference program's by a relative error of at most 0.014.
Values may be sent and summed in bfloat16 or wider, within the bound.
A program may use at most 128 MiB of HBM per device.

```python
import math
import jax
import jax.numpy as jnp
import numpy as np
from jax import lax

D = 2048
HEADS = 8
HEAD_DIM = 64
FFE = 512
SHARED_FF = 512
TOPK = 4
TOK_DEV = 128
TOK_SP = 1024
TOKEN_COUNT = 16384
EXPERTS = 256
CAP = 3
N_SP = 16
N_TP = 8


def head_law(key):
    base_key = jax.random.fold_in(key, 11)
    direction_key, choice_key, quick_key, gentle_key = jax.random.split(base_key, 4)
    direction = jax.random.normal(direction_key, (HEADS, HEAD_DIM), jnp.float32)
    direction = direction / jnp.sqrt(jnp.sum(direction * direction, axis=1, keepdims=True))
    gentle_share = 0.5
    gentle = jax.random.uniform(choice_key, (HEADS,), jnp.float32) < gentle_share
    quick_rate = jnp.exp(jax.random.uniform(quick_key, (HEADS,), jnp.float32, math.log(3.3), math.log(4.6)))
    gentle_rate = math.log(TOKEN_COUNT) + jax.random.uniform(gentle_key, (HEADS,), jnp.float32, 0.0, 0.8)
    intensity = jnp.where(gentle, gentle_rate, quick_rate)
    return (direction, intensity)


def draw_queries(key, part):
    direction, intensity = head_law(key)
    noise = jnp.clip(jax.random.normal(jax.random.fold_in(key, 21), (TOKEN_COUNT, HEADS, HEAD_DIM), jnp.float32), -3.0, 3.0)
    lifted = jnp.sqrt(intensity * math.sqrt(HEAD_DIM))
    drawn = 0.5 * noise + lifted[None, :, None] * direction[None]
    return drawn.reshape(TOKEN_COUNT, HEADS * HEAD_DIM).astype(jnp.bfloat16)


def draw_key_heads(key, part):
    direction, intensity = head_law(key)
    jitter_random_key, shift_random_key, spike_random_key = jax.random.split(jax.random.fold_in(key, 31), 3)
    noise = jnp.clip(jax.random.normal(jitter_random_key, (TOKEN_COUNT, HEADS, HEAD_DIM), jnp.float32), -3.0, 3.0)
    shift_values = jax.random.uniform(shift_random_key, (TOKEN_COUNT // TOK_SP,), jnp.float32, -0.5, 0.5)
    shift_values = jnp.repeat(shift_values, TOK_SP)
    spike_amount = jax.random.uniform(spike_random_key, (TOKEN_COUNT,), jnp.float32) < 6.0 / TOKEN_COUNT
    lifted = jnp.sqrt(intensity * math.sqrt(HEAD_DIM))
    multiplier = jnp.where(spike_amount[:, None], 0.8 / intensity[None, :], 1.0 + shift_values[:, None] / intensity[None, :])
    drawn = 0.5 * noise - (lifted[None, :] * multiplier)[:, :, None] * direction[None]
    return drawn.reshape(TOKEN_COUNT, HEADS * HEAD_DIM).astype(jnp.bfloat16)


def levels(rng, extent, cuts, least, high):
    factor_of, own = 1.0, jax.random.fold_in(rng, 6)
    for position, shards_of in cuts:
        heights = jnp.exp(jax.random.uniform(jax.random.fold_in(own, position), (shards_of,), jnp.float32, least / len(cuts), high / len(cuts)))
        factor_of = factor_of * jnp.repeat(heights, extent[position] // shards_of).reshape([-1 if axis == position else 1 for axis in range(len(extent))])
    return factor_of


def assign_block(key, own, number, rows, number_of, top, reach, skew):
    order = jax.random.permutation(key, number_of)
    heavy_load, usual = load_shares(number_of, rows * top, reach, skew, True), load_shares(number_of, rows * top, reach, skew, False)
    places = jnp.arange(number_of)

    def named(tallies, turn):
        used = int((tallies > 0).sum())
        fixed = max(1, used // 4)
        shifted = fixed + (places - fixed + turn * (used - fixed)) % max(1, number_of - fixed)
        return jnp.zeros((number_of,), jnp.int32).at[order[jnp.where(places < fixed, places, shifted)]].set(jnp.asarray(tallies, jnp.int32))

    tallies = jnp.where(number % 4 == 0, named(heavy_load, number // 4), named(usual, number - number // 4 - 1))
    mixed = jax.random.permutation(jax.random.fold_in(own, 3), number_of)
    source_of, receiver = mixed[0:number_of // 2 * 2:2], mixed[1:number_of // 2 * 2:2]
    room = jnp.minimum(tallies[source_of] - 1, reach - tallies[receiver]) // 2
    room = jnp.where((source_of == order[0]) | (receiver == order[0]) | (tallies[receiver] == 0), 0, jnp.maximum(room, 0))
    shifted = jax.random.randint(jax.random.fold_in(own, 4), (number_of // 2,), 0, 1 << 20) % (room + 1)
    tallies = tallies.at[source_of].add(-shifted).at[receiver].add(shifted)
    labels = jnp.searchsorted(jnp.cumsum(tallies), jnp.arange(rows * top), side="right").astype(jnp.int32)
    grid = labels.reshape(top, rows).T
    grid = grid[jax.random.permutation(jax.random.fold_in(own, 1), rows)]
    turn = jax.random.randint(jax.random.fold_in(own, 2), (rows, 1), 0, top)
    return jnp.take_along_axis(grid, (jnp.arange(top)[None, :] + turn) % top, axis=1)


def load_shares(number_of, total, bound, lean, full):
    loads = [(1 << 20) // math.isqrt(rank ** lean) + 1 for rank in range(1, number_of + 1)]
    largest = bound if full else min(bound, max(-(-total // number_of), total * loads[0] // sum(loads)))
    least = 1 if total - largest >= number_of - 1 else 0
    holding, rest = [largest] + [least] * (number_of - 1), total - largest - least * (number_of - 1)
    while rest > 0:
        free = [i for i in range(1, number_of) if holding[i] < largest] or [i for i in range(1, number_of) if holding[i] < bound]
        pool, left = sum([loads[i] for i in free]), rest
        for i in free:
            extra = min(bound - holding[i], max(1, left * loads[i] // pool), rest)
            holding[i] = holding[i] + extra
            rest = rest - extra
    return np.array(holding)


def gaussian(rng, extent, scale, limit, cuts=(), kind=jnp.bfloat16):
    result = scale * jax.random.normal(rng, extent, jnp.float32)
    if cuts:
        result = result * levels(rng, extent, cuts, -0.22, 0.18)
    return jnp.clip(result, -limit, limit).astype(kind)


def setup_inputs(seed: int = 0) -> dict:
    key_of = jax.random.split(jax.random.key(seed), 16)
    queries = draw_queries(jax.random.fold_in(key_of[15], 71), 0)
    key_heads = draw_key_heads(jax.random.fold_in(key_of[15], 71), 0)
    value_heads = gaussian(key_of[2], (TOKEN_COUNT, HEADS * HEAD_DIM), 1.0, 6.0, ((0, 16), (1, 8)))
    head_gain = jnp.clip(1.0 + 0.18 * jax.random.normal(key_of[3], (HEADS * HEAD_DIM,), jnp.float32), 0.1, 1.9)
    residual = gaussian(key_of[4], (TOKEN_COUNT, D), 1.0, 6.0, ((0, 128),))
    out_weight = gaussian(key_of[5], (HEADS * HEAD_DIM, D), (HEADS * HEAD_DIM) ** -0.5, 0.25)
    norm_gain = jnp.clip(1.0 + 0.18 * jax.random.normal(key_of[6], (D,), jnp.float32), 0.1, 1.9)
    shared_gate = gaussian(key_of[7], (D, SHARED_FF), D ** -0.5, 0.125)
    shared_up = gaussian(key_of[8], (D, SHARED_FF), D ** -0.5, 0.125)
    shared_down = gaussian(key_of[9], (SHARED_FF, D), SHARED_FF ** -0.5, 0.25)
    expert_gate = gaussian(key_of[10], (EXPERTS, D, FFE), D ** -0.5, 0.125, ((0, 128),))
    expert_up = gaussian(key_of[11], (EXPERTS, D, FFE), D ** -0.5, 0.125, ((0, 128),))
    expert_down = gaussian(key_of[12], (EXPERTS, FFE, D), FFE ** -0.5, 0.25, ((0, 128),))
    routed_experts_keys = jax.random.split(jax.random.fold_in(key_of[13], 1), TOKEN_COUNT // TOK_DEV)
    routed_experts_turns = jax.random.permutation(jax.random.fold_in(key_of[13], 3), TOKEN_COUNT // TOK_DEV)
    routed_experts = jax.vmap(lambda own, number: assign_block(jax.random.fold_in(key_of[13], 2), own, number, TOK_DEV, EXPERTS, TOPK, CAP, 2))(routed_experts_keys, routed_experts_turns).reshape((TOKEN_COUNT, TOPK))
    route_weights = jnp.clip(jnp.exp(math.log(1.5) - 2.7080502 * jax.random.uniform(key_of[14], (TOKEN_COUNT, TOPK), jnp.float32) ** levels(key_of[14], (TOKEN_COUNT, TOPK), ((0, 128),), -0.2, 0.2)), 0.1, 1.5)
    return dict(queries=queries, key_heads=key_heads, value_heads=value_heads, head_gain=head_gain, residual=residual, out_weight=out_weight, norm_gain=norm_gain, shared_gate=shared_gate, shared_up=shared_up, shared_down=shared_down, expert_gate=expert_gate, expert_up=expert_up, expert_down=expert_down, routed_experts=routed_experts, route_weights=route_weights)


EPSILON = 1e-06

def block_terms(query_block, key_block, value_block, query_start, key_start):
    scale = 1.0 / math.sqrt(HEAD_DIM)
    scores = jnp.einsum('qhd,khd->hqk', query_block.astype(jnp.float32), key_block.astype(jnp.float32)) * scale
    query_places = query_start + lax.iota(jnp.int32, query_block.shape[0])
    key_places = key_start + lax.iota(jnp.int32, key_block.shape[0])
    earlier = (key_places[None, :] < query_places[:, None])[None]
    stay_log = jnp.where(earlier, jax.nn.log_sigmoid(-scores), 0.0)
    after_log = lax.cumsum(stay_log, axis=2, reverse=True) - stay_log
    weights = jnp.where(earlier, jnp.exp(jax.nn.log_sigmoid(scores) + after_log), 0.0).astype(jnp.bfloat16)
    partial_out = jnp.einsum('hqk,khd->qhd', weights.astype(jnp.float32), value_block.astype(jnp.float32))
    block_total = jnp.transpose(lax.optimization_barrier(jnp.sum(stay_log, axis=2)))
    return (block_total, partial_out)

def head_norm(mixed, head_gain):
    inverse = lax.rsqrt(lax.optimization_barrier(jnp.mean(mixed * mixed, axis=2, keepdims=True)) + EPSILON)
    normed = mixed * inverse * head_gain.reshape(mixed.shape[1], mixed.shape[2])
    return normed.reshape(mixed.shape[0], -1).astype(jnp.bfloat16)

def stick_breaking(queries, key_heads, value_heads):
    query_width = 512 if TOK_SP % 512 == 0 else TOK_SP
    query_all = queries.reshape(TOKEN_COUNT // query_width, query_width, HEADS, HEAD_DIM)
    key_all = key_heads.reshape(N_SP, TOK_SP, HEADS, HEAD_DIM)
    value_all = value_heads.reshape(N_SP, TOK_SP, HEADS, HEAD_DIM)

    def one_block(block_index):
        query_block = lax.dynamic_index_in_dim(query_all, block_index, 0, keepdims=False)
        query_start = block_index * query_width

        def one_shard(running, shard_index):
            key_start = shard_index * TOK_SP

            def compute(unused):
                key_block = lax.dynamic_index_in_dim(key_all, shard_index, 0, keepdims=False)
                value_block = lax.dynamic_index_in_dim(value_all, shard_index, 0, keepdims=False)
                return block_terms(query_block, key_block, value_block, query_start, key_start)

            def nothing(unused):
                return (jnp.zeros((query_width, HEADS), jnp.float32), jnp.zeros((query_width, HEADS, HEAD_DIM), jnp.float32))
            return (running, lax.cond(key_start < query_start + query_width, compute, nothing, 0))
        leftover, stacked = lax.scan(one_shard, jnp.int32(0), jnp.arange(N_SP, dtype=jnp.int32))
        totals, partials = stacked
        later = lax.cumsum(totals, axis=0, reverse=True) - totals
        return lax.optimization_barrier(jnp.sum(jnp.exp(later)[..., None] * partials, axis=0))
    mixed = lax.map(one_block, jnp.arange(TOKEN_COUNT // query_width, dtype=jnp.int32))
    return mixed.reshape(TOKEN_COUNT, HEADS, HEAD_DIM)

def expert_block(inputs):
    expert_rows, gate_weight, up_weight, down_weight = inputs
    gate_part = jnp.dot(expert_rows, gate_weight, preferred_element_type=jnp.float32)
    up_part = jnp.dot(expert_rows, up_weight, preferred_element_type=jnp.float32)
    hidden = (jax.nn.silu(gate_part) * up_part).astype(jnp.bfloat16)
    return jnp.dot(hidden, down_weight, preferred_element_type=jnp.float32).astype(jnp.bfloat16)

def routed_sum(expert_input, expert_gate, expert_up, expert_down, routed_experts, route_weights):
    device_count = N_SP * N_TP
    flat_experts = routed_experts.reshape(-1)
    expert_table = (flat_experts[:, None] == jnp.arange(EXPERTS, dtype=jnp.int32)[None, :]).astype(jnp.int32)
    expert_table = expert_table.reshape(device_count, TOK_DEV * TOPK, EXPERTS)
    ranking = (lax.optimization_barrier(jnp.sum(jnp.cumsum(expert_table, axis=1) * expert_table, axis=2)) - 1).reshape(-1)
    source = jnp.arange(TOKEN_COUNT * TOPK, dtype=jnp.int32) // (TOK_DEV * TOPK)
    slot_index = (flat_experts * device_count + source) * CAP + ranking
    repeated = jnp.repeat(expert_input, TOPK, axis=0)
    buffer = jnp.zeros((EXPERTS * device_count * CAP, D), jnp.bfloat16).at[slot_index].set(repeated)
    buffer = buffer.reshape(EXPERTS, device_count * CAP, D)
    results = lax.map(expert_block, (buffer, expert_gate, expert_up, expert_down)).reshape(-1, D)
    slot_grid = slot_index.reshape(TOKEN_COUNT, TOPK)
    routed = jnp.zeros((TOKEN_COUNT, D), jnp.float32)
    for choice_index in range(TOPK):
        picked = results[slot_grid[:, choice_index]].astype(jnp.float32)
        routed = routed + picked * route_weights[:, choice_index][:, None]
    return routed

def reference(queries, key_heads, value_heads, head_gain, residual, out_weight, norm_gain, shared_gate, shared_up, shared_down, expert_gate, expert_up, expert_down, routed_experts, route_weights):
    head_output = head_norm(stick_breaking(queries, key_heads, value_heads), head_gain)
    branch = jnp.dot(head_output, out_weight, preferred_element_type=jnp.float32)
    stream = (residual.astype(jnp.float32) + branch).astype(jnp.bfloat16)
    stream_wide = stream.astype(jnp.float32)
    inverse = lax.rsqrt(lax.optimization_barrier(jnp.mean(stream_wide * stream_wide, axis=1, keepdims=True)) + EPSILON)
    expert_input = (stream_wide * inverse * norm_gain).astype(jnp.bfloat16)
    shared_hidden = (jax.nn.silu(jnp.dot(expert_input, shared_gate, preferred_element_type=jnp.float32)) * jnp.dot(expert_input, shared_up, preferred_element_type=jnp.float32)).astype(jnp.bfloat16)
    shared_term = jnp.dot(shared_hidden, shared_down, preferred_element_type=jnp.float32)
    routed = routed_sum(expert_input, expert_gate, expert_up, expert_down, routed_experts, route_weights)
    return (stream_wide + shared_term + routed).astype(jnp.bfloat16)
```

```python
import math

import jax
import jax.numpy as jnp
from jax import lax
from jax.experimental import pallas as pl
from jax.experimental.pallas import tpu as pltpu
from jax.sharding import PartitionSpec as P

HEAD_DIM = 64


EPSILON = 1e-06


LOG2E = 1.4426950408889634
TILE = 256


def tile_terms(q2, keys, values, tri, carry, mask):
    x = jnp.dot(q2, keys, preferred_element_type=jnp.float32)
    drop = jnp.maximum(jnp.log(1.0 + jnp.exp2(jnp.minimum(x, 126.0))) * LOG2E, x)
    stick = x - drop
    if mask is not None:
        drop = jnp.where(mask, drop, 0.0)
    after = jnp.dot(drop.astype(jnp.bfloat16), tri, preferred_element_type=jnp.float32)
    both = jnp.concatenate([carry, carry], axis=1)
    weights = jnp.exp2(stick - after - both)
    if mask is not None:
        weights = jnp.where(mask, weights, 0.0)
    out = jnp.dot(weights.astype(jnp.bfloat16), values, preferred_element_type=jnp.float32)
    total = after[:, :1] + drop[:, :1]
    return out, carry + jnp.broadcast_to(total, carry.shape)


def attention_kernel(q_ref, kv_ref, gain_ref, out_ref, q2_ref, acc_ref, carry_ref, tri_ref):
    me = lax.axis_index("sp")
    q = q_ref[...].astype(jnp.float32) * (LOG2E / math.sqrt(HEAD_DIM))
    high = q.astype(jnp.bfloat16)
    low = (q - high.astype(jnp.float32)).astype(jnp.bfloat16)
    q2_ref[...] = jnp.concatenate([high, low], axis=1)
    row = lax.broadcasted_iota(jnp.int32, (TILE, TILE), 0)
    column = lax.broadcasted_iota(jnp.int32, (TILE, TILE), 1)
    tri_ref[...] = (row > column).astype(jnp.float32).astype(jnp.bfloat16)
    acc_ref[...] = jnp.zeros_like(acc_ref)
    carry_ref[...] = jnp.zeros_like(carry_ref)
    tiles = q_ref.shape[0] // TILE

    def chunk(block, part):
        left = kv_ref[block, pl.ds(part * 128, 64), :]
        right = kv_ref[block, pl.ds(part * 128 + 64, 64), :]
        keys = jnp.concatenate([left, right], axis=1)
        keys = jnp.concatenate([keys, keys], axis=0)
        values = kv_ref[block, pl.ds(512 + (part % 2) * TILE, TILE), :]
        side = lax.broadcasted_iota(jnp.int32, values.shape, 1) // HEAD_DIM
        return keys, jnp.where(side == part // 2, values, jnp.zeros_like(values))

    def add(tile, keys, values, mask):
        rows = pl.ds(tile * TILE, TILE)
        out, carry = tile_terms(
            q2_ref[rows, :], keys, values, tri_ref[...], carry_ref[rows, :], mask
        )
        acc_ref[rows, :] += out
        carry_ref[rows, :] = carry

    for part in range(tiles - 1, -1, -1):
        keys, values = chunk(me, part)
        for tile in range(part, tiles):
            add(tile, keys, values, column < row if tile == part else None)

    def step(i, unused):
        keys, values = chunk(me - 1 - i // tiles, tiles - 1 - i % tiles)
        for tile in range(tiles):
            add(tile, keys, values, None)
        return unused

    lax.fori_loop(0, me * tiles, step, 0)
    mixed = acc_ref[:, :HEAD_DIM] + acc_ref[:, HEAD_DIM:]
    inverse = lax.rsqrt(jnp.mean(mixed * mixed, axis=1, keepdims=True) + EPSILON)
    out_ref[...] = (mixed * inverse * gain_ref[...]).astype(jnp.bfloat16)


def pack_keys_values(key_heads, value_heads):
    rows = key_heads.shape[0]
    keys = key_heads.reshape(rows // 128, 128, HEAD_DIM).transpose(0, 2, 1).reshape(-1, 128)
    values = value_heads.reshape(2, rows // 2, HEAD_DIM).transpose(1, 0, 2).reshape(-1, 128)
    return jnp.concatenate([keys, values], axis=0)


def attention(queries, key_heads, value_heads, head_gain):
    rows = queries.shape[0]
    packed = pack_keys_values(key_heads, value_heads)
    everyone = lax.all_gather(packed, "sp", axis=0, tiled=False)
    return pl.pallas_call(
        attention_kernel,
        out_shape=jax.ShapeDtypeStruct((rows, HEAD_DIM), jnp.bfloat16),
        in_specs=[pl.BlockSpec(memory_space=pltpu.VMEM)] * 3,
        out_specs=pl.BlockSpec(memory_space=pltpu.VMEM),
        scratch_shapes=[
            pltpu.VMEM((rows, 128), jnp.bfloat16),
            pltpu.VMEM((rows, 128), jnp.float32),
            pltpu.VMEM((rows, 128), jnp.float32),
            pltpu.VMEM((TILE, TILE), jnp.bfloat16),
        ],
        compiler_params=pltpu.CompilerParams(vmem_limit_bytes=40 << 20),
        name="attention",
    )(queries, everyone, head_gain.reshape(1, HEAD_DIM))


def routed_sum(expert_input, expert_gate, expert_up, expert_down, routed_experts, route_weights):
    row_count, pick_count = routed_experts.shape
    local_experts = expert_gate.shape[0]
    model_width = expert_input.shape[1]
    sp_count = lax.axis_size("sp")
    tp_count = lax.axis_size("tp")
    device_count = sp_count * tp_count
    expert_count = local_experts * device_count
    capacity = max(2, 3 * row_count * pick_count // (2 * expert_count))
    flat_experts = routed_experts.reshape(-1)
    expert_table = (
        flat_experts[:, None] == jnp.arange(expert_count, dtype=jnp.int32)[None, :]
    ).astype(jnp.int32)
    ranking = jnp.sum(jnp.cumsum(expert_table, axis=0) * expert_table, axis=1) - 1
    holder = flat_experts // local_experts
    resident = flat_experts % local_experts
    slot_index = (resident * device_count + holder) * capacity + ranking
    placement = (
        slot_index[:, None] == jnp.arange(expert_count * capacity, dtype=jnp.int32)[None, :]
    ).astype(jnp.bfloat16)
    token_place = jnp.sum(placement.reshape(row_count, pick_count, -1), axis=1)
    outgoing = jnp.einsum(
        "rs,rd->sd", token_place, expert_input, preferred_element_type=jnp.float32
    ).astype(jnp.bfloat16)
    outgoing = outgoing.reshape(local_experts, device_count, capacity, model_width)
    arrived = lax.all_to_all(outgoing, ("sp", "tp"), split_axis=1, concat_axis=1, tiled=True)
    grouped = arrived.reshape(local_experts, -1, model_width)
    gate_part = jnp.einsum("erd,edf->erf", grouped, expert_gate, preferred_element_type=jnp.float32)
    up_part = jnp.einsum("erd,edf->erf", grouped, expert_up, preferred_element_type=jnp.float32)
    hidden = (jax.nn.silu(gate_part) * up_part).astype(jnp.bfloat16)
    result = jnp.einsum(
        "erf,efd->erd", hidden, expert_down, preferred_element_type=jnp.float32
    ).astype(jnp.bfloat16)
    returned = lax.all_to_all(
        result.reshape(arrived.shape), ("sp", "tp"), split_axis=1, concat_axis=1, tiled=True
    )
    gathered = jnp.dot(
        placement, returned.reshape(-1, model_width), preferred_element_type=jnp.float32
    )
    weighted = gathered.reshape(row_count, pick_count, model_width) * route_weights[:, :, None]
    return jnp.sum(weighted, axis=1)


def body(
    queries,
    key_heads,
    value_heads,
    head_gain,
    residual,
    out_weight,
    norm_gain,
    shared_gate,
    shared_up,
    shared_down,
    expert_gate,
    expert_up,
    expert_down,
    routed_experts,
    route_weights,
):
    head_output = attention(queries, key_heads, value_heads, head_gain)
    token_heads = lax.all_to_all(head_output, "tp", split_axis=0, concat_axis=1, tiled=True)
    branch = jnp.dot(token_heads, out_weight, preferred_element_type=jnp.float32)
    stream = (residual.astype(jnp.float32) + branch).astype(jnp.bfloat16)
    stream_wide = stream.astype(jnp.float32)
    inverse = lax.rsqrt(jnp.mean(stream_wide * stream_wide, axis=1, keepdims=True) + EPSILON)
    expert_input = (stream_wide * inverse * norm_gain).astype(jnp.bfloat16)
    shared_hidden = (
        jax.nn.silu(jnp.dot(expert_input, shared_gate, preferred_element_type=jnp.float32))
        * jnp.dot(expert_input, shared_up, preferred_element_type=jnp.float32)
    ).astype(jnp.bfloat16)
    shared_term = jnp.dot(shared_hidden, shared_down, preferred_element_type=jnp.float32)
    routed = routed_sum(
        expert_input, expert_gate, expert_up, expert_down, routed_experts, route_weights
    )
    return (stream_wide + shared_term + routed).astype(jnp.bfloat16)


def solution(mesh):
    return jax.shard_map(
        body,
        mesh=mesh,
        in_specs=(
            P("sp", "tp"),
            P("sp", "tp"),
            P("sp", "tp"),
            P("tp"),
            P(("sp", "tp"), None),
            P(),
            P(),
            P(),
            P(),
            P(),
            P(("sp", "tp"), None, None),
            P(("sp", "tp"), None, None),
            P(("sp", "tp"), None, None),
            P(("sp", "tp"), None),
            P(("sp", "tp"), None),
        ),
        out_specs=P(("sp", "tp"), None),
        check_vma=False,
    )
```

```python
import math

import jax
import jax.numpy as jnp
from jax import lax
from jax.experimental import pallas as pl
from jax.experimental.pallas import tpu as pltpu
from jax.sharding import PartitionSpec as P

HEAD_DIM = 64


EPSILON = 1e-06


LOG2E = 1.4426950408889634
TILE = 256
MESH = pl.DeviceIdType.MESH


def tile_terms(q2, keys, values, tri, carry, mask):
    x = jnp.dot(q2, keys, preferred_element_type=jnp.float32)
    drop = jnp.maximum(jnp.log(1.0 + jnp.exp2(jnp.minimum(x, 126.0))) * LOG2E, x)
    stick = x - drop
    if mask is not None:
        drop = jnp.where(mask, drop, 0.0)
    after = jnp.dot(drop.astype(jnp.bfloat16), tri, preferred_element_type=jnp.float32)
    both = jnp.concatenate([carry, carry], axis=1)
    weights = jnp.exp2(stick - after - both)
    if mask is not None:
        weights = jnp.where(mask, weights, 0.0)
    out = jnp.dot(weights.astype(jnp.bfloat16), values, preferred_element_type=jnp.float32)
    total = after[:, :1] + drop[:, :1]
    return out, carry + jnp.broadcast_to(total, carry.shape)


def attention_kernel(
    q_ref, k_ref, v_ref, gain_ref, out_ref,
    q_own, q_ref2, key_ref, value_ref, acc_ref, carry_ref, tri_ref, out_own, out_in,
    q_send, q_recv, q_local, send_sem, key_recv, value_recv, out_send, out_recv, out_local,
):
    me, head = lax.axis_index("sp"), lax.axis_index("tp")
    row, column = me // 4, me % 4
    half = q_ref.shape[0] // 2

    q = q_ref[...].astype(jnp.float32) * (LOG2E / math.sqrt(HEAD_DIM))
    high = q.astype(jnp.bfloat16)
    low = (q - high.astype(jnp.float32)).astype(jnp.bfloat16)
    both = jnp.concatenate([high, low], axis=1)
    q_own[0] = both[:half]
    q_own[1] = both[half:]
    for part in range(8):
        block = k_ref[pl.ds(part * 128, 128), :].astype(jnp.float32)
        key_ref[me, pl.ds(part * HEAD_DIM, HEAD_DIM), :] = block.T.astype(jnp.bfloat16)
    v = v_ref[...].astype(jnp.float32)
    value_ref[me] = jnp.concatenate([v[:half], v[half:]], axis=1).astype(jnp.bfloat16)

    def copy(source, target, out_sem, in_sem, where, which):
        return pltpu.make_async_remote_copy(
            src_ref=source, dst_ref=target, send_sem=out_sem, recv_sem=in_sem,
            device_id=(where, which), device_id_type=MESH,
        )

    slot = jnp.where(me < 8, 1, 0)
    for part in range(2):
        place = 2 * me + part
        owner = jnp.where(place < 16, place, 31 - place)

        @pl.when(owner != me)
        def _():
            copy(q_own.at[part], q_ref2.at[slot], q_send.at[part], q_recv.at[slot], owner, head).start()

        @pl.when(owner == me)
        def _():
            pltpu.make_async_copy(q_own.at[part], q_ref2.at[slot], q_local).start()

    steps = (1, 3, 2)

    def key_copy(block, n, where):
        return copy(key_ref.at[block], key_ref.at[block], send_sem.at[n], key_recv.at[block], where, head)

    def value_copy(block, n, where):
        return copy(value_ref.at[block], value_ref.at[block], send_sem.at[n], value_recv.at[block], where, head)

    along = [row * 4 + (column + d) % 4 for d in steps]
    across = [(row + d) % 4 * 4 + column for d in steps]
    sent = []
    for n in range(3):
        sent.append(key_copy(me, n, along[n]))
        sent.append(value_copy(me, 3 + n, across[n]))
    for n in range(3):
        sent.append(key_copy(me, 6 + n, across[n]))
        sent.append(value_copy(me, 9 + n, along[n]))
    for one in sent:
        one.start()

    r = lax.broadcasted_iota(jnp.int32, (TILE, TILE), 0)
    c = lax.broadcasted_iota(jnp.int32, (TILE, TILE), 1)
    tri_ref[...] = (r > c).astype(jnp.float32).astype(jnp.bfloat16)
    acc_ref[...] = jnp.zeros_like(acc_ref)
    carry_ref[...] = jnp.zeros_like(carry_ref)

    for n in range(3):
        key_copy(along[n], 0, me).wait_recv()
        for m in range(3):
            one = key_copy(along[n], 12 + 3 * n + m, across[m])
            one.start()
            sent.append(one)
        value_copy(across[n], 0, me).wait_recv()
        for m in range(3):
            one = value_copy(across[n], 21 + 3 * n + m, along[m])
            one.start()
            sent.append(one)

    def arrived(block):
        @pl.when(block // 4 != row)
        def _():
            key_copy(block, 0, me).wait_recv()

        @pl.when(block % 4 != column)
        def _():
            value_copy(block, 0, me).wait_recv()

    def unit(which, place, diagonal):
        block, side = place // 2, place % 2
        for part in (1, 0):
            at = (2 * side + part) * 128
            left = key_ref[block, pl.ds(at, HEAD_DIM), :]
            right = key_ref[block, pl.ds(at + HEAD_DIM, HEAD_DIM), :]
            keys = jnp.concatenate([left, right], axis=1)
            keys = jnp.concatenate([keys, keys], axis=0)
            values = value_ref[block, pl.ds(part * TILE, TILE), :]
            lanes = lax.broadcasted_iota(jnp.int32, values.shape, 1) // HEAD_DIM
            values = jnp.where(lanes == side, values, jnp.zeros_like(values))
            for tile in range(2):
                if diagonal and tile < part:
                    continue
                rows = pl.ds(tile * TILE, TILE)
                mask = c < r if diagonal and tile == part else None
                out, carry = tile_terms(
                    q_ref2[which, rows, :], keys, values, tri_ref[...], carry_ref[which, rows, :], mask
                )
                acc_ref[which, rows, :] += out
                carry_ref[which, rows, :] = carry

    def finish(which, place):
        acc = acc_ref[which]
        mixed = acc[:, :HEAD_DIM] + acc[:, HEAD_DIM:]
        inverse = lax.rsqrt(jnp.mean(mixed * mixed, axis=1, keepdims=True) + EPSILON)
        normed = mixed * inverse * gain_ref[...]
        for piece in range(4):
            at = piece * 128
            two = jnp.concatenate([normed[at : at + 64], normed[at + 64 : at + 128]], axis=1)
            out_own[4 * which + piece] = two.astype(jnp.bfloat16)
        for piece in range(4):
            n = 4 * which + piece
            where, token = place // 2, (place % 2) * 4 + piece
            mine = (where == me) & (token == head)

            @pl.when(jnp.logical_not(mine))
            def _():
                copy(out_own.at[n], out_in.at[head], out_send.at[n], out_recv.at[head], where, token).start()

            @pl.when(mine)
            def _():
                pltpu.make_async_copy(out_own.at[n], out_in.at[head], out_local).start()

    @pl.when(me != 10)
    def _():
        copy(q_own.at[0], q_ref2.at[0], q_send.at[0], q_recv.at[0], me, head).wait_recv()

    @pl.when(me != 0)
    def _():
        copy(q_own.at[0], q_ref2.at[1], q_send.at[0], q_recv.at[1], me, head).wait_recv()

    @pl.when((me == 0) | (me == 10))
    def _():
        pltpu.make_async_copy(q_own.at[0], q_ref2.at[0], q_local).wait()

    far = 31 - me
    arrived(far // 2)
    unit(0, far, True)

    def far_step(n, unused):
        place = far - 1 - n

        @pl.when(place % 2 == 1)
        def _():
            arrived(place // 2)

        unit(0, place, False)
        return unused

    lax.fori_loop(0, far, far_step, 0)
    finish(0, far)
    unit(1, me, True)

    def near_step(n, unused):
        unit(1, me - 1 - n, False)
        return unused

    lax.fori_loop(0, me, near_step, 0)
    finish(1, me)

    def drain(n, unused):
        arrived(n)
        return unused

    lax.fori_loop(far // 2 + 1, 16, drain, 0)
    for part in range(2):
        place = 2 * me + part
        owner = jnp.where(place < 16, place, 31 - place)

        @pl.when(owner != me)
        def _():
            copy(q_own.at[part], q_ref2.at[slot], q_send.at[part], q_recv.at[slot], owner, head).wait_send()
    for one in sent:
        one.wait_send()

    place = 2 * me + head // 4
    owner = jnp.where(place < 16, place, 31 - place)
    for other in range(8):
        @pl.when(jnp.logical_not((owner == me) & (other == head)))
        def _():
            copy(out_own.at[0], out_in.at[other], out_send.at[0], out_recv.at[other], me, head).wait_recv()
    for which, spot in ((0, far), (1, me)):
        for piece in range(4):
            n = 4 * which + piece
            where, token = spot // 2, (spot % 2) * 4 + piece
            mine = (where == me) & (token == head)

            @pl.when(jnp.logical_not(mine))
            def _():
                copy(out_own.at[n], out_in.at[head], out_send.at[n], out_recv.at[head], where, token).wait_send()

            @pl.when(mine)
            def _():
                pltpu.make_async_copy(out_own.at[n], out_in.at[head], out_local).wait()

    for pair in range(4):
        one = out_in[2 * pair].astype(jnp.float32)
        two = out_in[2 * pair + 1].astype(jnp.float32)
        one = jnp.concatenate([one[:, :HEAD_DIM], one[:, HEAD_DIM:]], axis=0)
        two = jnp.concatenate([two[:, :HEAD_DIM], two[:, HEAD_DIM:]], axis=0)
        out_ref[:, pl.ds(pair * 128, 128)] = jnp.concatenate([one, two], axis=1).astype(jnp.bfloat16)


def attention(queries, key_heads, value_heads, head_gain):
    rows = queries.shape[0]
    half = rows // 2
    return pl.pallas_call(
        attention_kernel,
        out_shape=jax.ShapeDtypeStruct((128, 8 * HEAD_DIM), jnp.bfloat16),
        in_specs=[pl.BlockSpec(memory_space=pltpu.VMEM)] * 4,
        out_specs=pl.BlockSpec(memory_space=pltpu.VMEM),
        scratch_shapes=[
            pltpu.VMEM((2, half, 128), jnp.bfloat16),
            pltpu.VMEM((2, half, 128), jnp.bfloat16),
            pltpu.VMEM((16, half, 128), jnp.bfloat16),
            pltpu.VMEM((16, half, 128), jnp.bfloat16),
            pltpu.VMEM((2, half, 128), jnp.float32),
            pltpu.VMEM((2, half, 128), jnp.float32),
            pltpu.VMEM((TILE, TILE), jnp.bfloat16),
            pltpu.VMEM((8, 64, 128), jnp.bfloat16),
            pltpu.VMEM((8, 64, 128), jnp.bfloat16),
            pltpu.SemaphoreType.DMA((2,)),
            pltpu.SemaphoreType.DMA((2,)),
            pltpu.SemaphoreType.DMA,
            pltpu.SemaphoreType.DMA((30,)),
            pltpu.SemaphoreType.DMA((16,)),
            pltpu.SemaphoreType.DMA((16,)),
            pltpu.SemaphoreType.DMA((8,)),
            pltpu.SemaphoreType.DMA((8,)),
            pltpu.SemaphoreType.DMA,
        ],
        compiler_params=pltpu.CompilerParams(vmem_limit_bytes=40 << 20, has_side_effects=True),
        name="attention",
    )(queries, key_heads, value_heads, head_gain.reshape(1, HEAD_DIM))


def routed_sum(expert_input, expert_gate, expert_up, expert_down, routed_experts, route_weights):
    row_count, pick_count = routed_experts.shape
    local_experts = expert_gate.shape[0]
    model_width = expert_input.shape[1]
    sp_count = lax.axis_size("sp")
    tp_count = lax.axis_size("tp")
    device_count = sp_count * tp_count
    expert_count = local_experts * device_count
    capacity = max(2, 3 * row_count * pick_count // (2 * expert_count))
    flat_experts = routed_experts.reshape(-1)
    expert_table = (
        flat_experts[:, None] == jnp.arange(expert_count, dtype=jnp.int32)[None, :]
    ).astype(jnp.int32)
    ranking = jnp.sum(jnp.cumsum(expert_table, axis=0) * expert_table, axis=1) - 1
    holder = flat_experts // local_experts
    resident = flat_experts % local_experts
    slot_index = (resident * device_count + holder) * capacity + ranking
    placement = (
        slot_index[:, None] == jnp.arange(expert_count * capacity, dtype=jnp.int32)[None, :]
    ).astype(jnp.bfloat16)
    token_place = jnp.sum(placement.reshape(row_count, pick_count, -1), axis=1)
    outgoing = jnp.einsum(
        "rs,rd->sd", token_place, expert_input, preferred_element_type=jnp.float32
    ).astype(jnp.bfloat16)
    outgoing = outgoing.reshape(local_experts, device_count, capacity, model_width)
    arrived = lax.all_to_all(outgoing, ("sp", "tp"), split_axis=1, concat_axis=1, tiled=True)
    grouped = arrived.reshape(local_experts, -1, model_width)
    gate_part = jnp.einsum("erd,edf->erf", grouped, expert_gate, preferred_element_type=jnp.float32)
    up_part = jnp.einsum("erd,edf->erf", grouped, expert_up, preferred_element_type=jnp.float32)
    hidden = (jax.nn.silu(gate_part) * up_part).astype(jnp.bfloat16)
    result = jnp.einsum(
        "erf,efd->erd", hidden, expert_down, preferred_element_type=jnp.float32
    ).astype(jnp.bfloat16)
    returned = lax.all_to_all(
        result.reshape(arrived.shape), ("sp", "tp"), split_axis=1, concat_axis=1, tiled=True
    )
    gathered = jnp.dot(
        placement, returned.reshape(-1, model_width), preferred_element_type=jnp.float32
    )
    weighted = gathered.reshape(row_count, pick_count, model_width) * route_weights[:, :, None]
    return jnp.sum(weighted, axis=1)


def body(
    queries,
    key_heads,
    value_heads,
    head_gain,
    residual,
    out_weight,
    norm_gain,
    shared_gate,
    shared_up,
    shared_down,
    expert_gate,
    expert_up,
    expert_down,
    routed_experts,
    route_weights,
):
    token_heads = attention(queries, key_heads, value_heads, head_gain)
    branch = jnp.dot(token_heads, out_weight, preferred_element_type=jnp.float32)
    stream = (residual.astype(jnp.float32) + branch).astype(jnp.bfloat16)
    stream_wide = stream.astype(jnp.float32)
    inverse = lax.rsqrt(jnp.mean(stream_wide * stream_wide, axis=1, keepdims=True) + EPSILON)
    expert_input = (stream_wide * inverse * norm_gain).astype(jnp.bfloat16)
    shared_hidden = (
        jax.nn.silu(jnp.dot(expert_input, shared_gate, preferred_element_type=jnp.float32))
        * jnp.dot(expert_input, shared_up, preferred_element_type=jnp.float32)
    ).astype(jnp.bfloat16)
    shared_term = jnp.dot(shared_hidden, shared_down, preferred_element_type=jnp.float32)
    routed = routed_sum(
        expert_input, expert_gate, expert_up, expert_down, routed_experts, route_weights
    )
    return (stream_wide + shared_term + routed).astype(jnp.bfloat16)


def solution(mesh):
    return jax.shard_map(
        body,
        mesh=mesh,
        in_specs=(
            P("sp", "tp"),
            P("sp", "tp"),
            P("sp", "tp"),
            P("tp"),
            P(("sp", "tp"), None),
            P(),
            P(),
            P(),
            P(),
            P(),
            P(("sp", "tp"), None, None),
            P(("sp", "tp"), None, None),
            P(("sp", "tp"), None, None),
            P(("sp", "tp"), None),
            P(("sp", "tp"), None),
        ),
        out_specs=P(("sp", "tp"), None),
        check_vma=False,
    )
```

```python
import math

import jax
import jax.numpy as jnp
from jax import lax
from jax.experimental import pallas as pl
from jax.experimental.pallas import tpu as pltpu
from jax.sharding import PartitionSpec as P

HEAD_DIM = 64


EPSILON = 1e-06


LOG2E = 1.4426950408889634
TILE = 256
MESH = pl.DeviceIdType.MESH


def tile_terms(q2, keys, values, tri, carry, mask):
    x = jnp.dot(q2, keys, preferred_element_type=jnp.float32)
    drop = jnp.maximum(jnp.log(1.0 + jnp.exp2(jnp.minimum(x, 126.0))) * LOG2E, x)
    stick = x - drop
    if mask is not None:
        drop = jnp.where(mask, drop, 0.0)
    after = jnp.dot(drop.astype(jnp.bfloat16), tri, preferred_element_type=jnp.float32)
    both = jnp.concatenate([carry, carry], axis=1)
    weights = jnp.exp2(stick - after - both)
    if mask is not None:
        weights = jnp.where(mask, weights, 0.0)
    out = jnp.dot(weights.astype(jnp.bfloat16), values, preferred_element_type=jnp.float32)
    total = after[:, :1] + drop[:, :1]
    return out, carry + jnp.broadcast_to(total, carry.shape)


def attention_kernel(
    q_ref, k_ref, v_ref, gain_ref, out_ref,
    q_own, q_ref2, key_ref, value_ref, acc_ref, carry_ref, sum_ref, past_ref, tri_ref, out_own, out_in,
    q_send, q_recv, q_local, send_sem, key_recv, value_recv, out_send, out_recv, out_local,
):
    me, head = lax.axis_index("sp"), lax.axis_index("tp")
    row, column = me // 4, me % 4
    half = q_ref.shape[0] // 2

    q = q_ref[...].astype(jnp.float32) * (LOG2E / math.sqrt(HEAD_DIM))
    high = q.astype(jnp.bfloat16)
    low = (q - high.astype(jnp.float32)).astype(jnp.bfloat16)
    both = jnp.concatenate([high, low], axis=1)
    q_own[0] = both[:half]
    q_own[1] = both[half:]
    for part in range(8):
        block = k_ref[pl.ds(part * 128, 128), :].astype(jnp.float32)
        key_ref[me, pl.ds(part * HEAD_DIM, HEAD_DIM), :] = block.T.astype(jnp.bfloat16)
    v = v_ref[...].astype(jnp.float32)
    value_ref[me] = jnp.concatenate([v[:half], v[half:]], axis=1).astype(jnp.bfloat16)

    def copy(source, target, out_sem, in_sem, where, which):
        return pltpu.make_async_remote_copy(
            src_ref=source, dst_ref=target, send_sem=out_sem, recv_sem=in_sem,
            device_id=(where, which), device_id_type=MESH,
        )

    slot = jnp.where(me < 8, 1, 0)
    for part in range(2):
        place = 2 * me + part
        owner = jnp.where(place < 16, place, 31 - place)

        @pl.when(owner != me)
        def _():
            copy(q_own.at[part], q_ref2.at[slot], q_send.at[part], q_recv.at[slot], owner, head).start()

        @pl.when(owner == me)
        def _():
            pltpu.make_async_copy(q_own.at[part], q_ref2.at[slot], q_local).start()

    steps = (1, 3, 2)

    def key_copy(block, n, where):
        return copy(key_ref.at[block], key_ref.at[block], send_sem.at[n], key_recv.at[block], where, head)

    def value_copy(block, n, where):
        return copy(value_ref.at[block], value_ref.at[block], send_sem.at[n], value_recv.at[block], where, head)

    along = [row * 4 + (column + d) % 4 for d in steps]
    across = [(row + d) % 4 * 4 + column for d in steps]
    sent = []
    for n in range(3):
        sent.append(key_copy(me, n, along[n]))
        sent.append(value_copy(me, 3 + n, across[n]))
    for n in range(3):
        sent.append(key_copy(me, 6 + n, across[n]))
        sent.append(value_copy(me, 9 + n, along[n]))
    for one in sent:
        one.start()

    r = lax.broadcasted_iota(jnp.int32, (TILE, TILE), 0)
    c = lax.broadcasted_iota(jnp.int32, (TILE, TILE), 1)
    tri_ref[...] = (r > c).astype(jnp.float32).astype(jnp.bfloat16)
    passed = []

    def forward():
        for n in range(3):
            key_copy(along[n], 0, me).wait_recv()
            for m in range(3):
                key_copy(along[n], 12 + 3 * n + m, across[m]).start()
            value_copy(across[n], 0, me).wait_recv()
            for m in range(3):
                value_copy(across[n], 21 + 3 * n + m, along[m]).start()

    for n in range(3):
        for m in range(3):
            passed.append(key_copy(along[n], 12 + 3 * n + m, across[m]))
            passed.append(value_copy(across[n], 21 + 3 * n + m, along[m]))

    def arrived(block):
        @pl.when(block // 4 != row)
        def _():
            key_copy(block, 0, me).wait_recv()

        @pl.when(block % 4 != column)
        def _():
            value_copy(block, 0, me).wait_recv()

    def unit(which, place, diagonal):
        block, side = place // 2, place % 2
        for part in (1, 0):
            at = (2 * side + part) * 128
            left = key_ref[block, pl.ds(at, HEAD_DIM), :]
            right = key_ref[block, pl.ds(at + HEAD_DIM, HEAD_DIM), :]
            keys = jnp.concatenate([left, right], axis=1)
            keys = jnp.concatenate([keys, keys], axis=0)
            values = value_ref[block, pl.ds(part * TILE, TILE), :]
            lanes = lax.broadcasted_iota(jnp.int32, values.shape, 1) // HEAD_DIM
            values = jnp.where(lanes == side, values, jnp.zeros_like(values))
            for tile in range(2):
                if diagonal and tile < part:
                    continue
                rows = pl.ds(tile * TILE, TILE)
                mask = c < r if diagonal and tile == part else None
                out, carry = tile_terms(
                    q_ref2[which, rows, :], keys, values, tri_ref[...], carry_ref[which, block, rows, :], mask
                )
                acc_ref[which, block, rows, :] += out
                carry_ref[which, block, rows, :] = carry

    def finish(which, place):
        blank = jnp.zeros((half, 128), jnp.float32)
        sum_ref[...] = blank
        past_ref[...] = blank

        def later(n, unused):
            block = place // 2 - n
            sum_ref[...] += jnp.exp2(-past_ref[...]) * acc_ref[which, block]
            past_ref[...] += carry_ref[which, block]
            return unused

        lax.fori_loop(0, place // 2 + 1, later, 0)
        acc = sum_ref[...]
        mixed = acc[:, :HEAD_DIM] + acc[:, HEAD_DIM:]
        inverse = lax.rsqrt(jnp.mean(mixed * mixed, axis=1, keepdims=True) + EPSILON)
        normed = mixed * inverse * gain_ref[...]
        for piece in range(4):
            at = piece * 128
            two = jnp.concatenate([normed[at : at + 64], normed[at + 64 : at + 128]], axis=1)
            out_own[4 * which + piece] = two.astype(jnp.bfloat16)
        for piece in range(4):
            n = 4 * which + piece
            where, token = place // 2, (place % 2) * 4 + piece
            mine = (where == me) & (token == head)

            @pl.when(jnp.logical_not(mine))
            def _():
                copy(out_own.at[n], out_in.at[head], out_send.at[n], out_recv.at[head], where, token).start()

            @pl.when(mine)
            def _():
                pltpu.make_async_copy(out_own.at[n], out_in.at[head], out_local).start()

    @pl.when(me != 10)
    def _():
        copy(q_own.at[0], q_ref2.at[0], q_send.at[0], q_recv.at[0], me, head).wait_recv()

    @pl.when(me != 0)
    def _():
        copy(q_own.at[0], q_ref2.at[1], q_send.at[0], q_recv.at[1], me, head).wait_recv()

    @pl.when((me == 0) | (me == 10))
    def _():
        pltpu.make_async_copy(q_own.at[0], q_ref2.at[0], q_local).wait()

    far = 31 - me
    order = ((0, 0), (0, 1), (1, 0), (0, 3), (3, 0), (0, 2), (2, 0), (1, 1), (3, 3), (1, 3), (3, 1), (1, 2), (2, 1), (3, 2), (2, 3), (2, 2))

    def pick(n, axis):
        return sum(jnp.where(n == k, one[axis], 0) for k, one in enumerate(order))

    def visit(n, unused):
        block = (row + pick(n, 0)) % 4 * 4 + (column + pick(n, 1)) % 4

        @pl.when(n == 1)
        def _():
            forward()

        @pl.when((block <= far // 2) & (n > 0))
        def _():
            arrived(block)

        def pair(i, unused):
            which, side = i // 2, 1 - i % 2
            top = jnp.where(which == 0, far, me)
            place = 2 * block + side

            @pl.when((side == 1) & (2 * block <= top))
            def _():
                acc_ref[which, block] = jnp.zeros((half, 128), jnp.float32)
                carry_ref[which, block] = jnp.zeros((half, 128), jnp.float32)

            @pl.when(place < top)
            def _():
                unit(which, place, False)

            @pl.when(place == top)
            def _():
                unit(which, place, True)

            return unused

        @pl.when(block <= far // 2)
        def _():
            lax.fori_loop(0, 4, pair, 0)

        return unused

    lax.fori_loop(0, 16, visit, 0)
    finish(0, far)
    finish(1, me)

    def drain(n, unused):
        @pl.when(n != me)
        def _():
            arrived(n)

        return unused

    lax.fori_loop(far // 2 + 1, 16, drain, 0)
    for part in range(2):
        place = 2 * me + part
        owner = jnp.where(place < 16, place, 31 - place)

        @pl.when(owner != me)
        def _():
            copy(q_own.at[part], q_ref2.at[slot], q_send.at[part], q_recv.at[slot], owner, head).wait_send()
    for one in sent + passed:
        one.wait_send()

    place = 2 * me + head // 4
    owner = jnp.where(place < 16, place, 31 - place)
    for other in range(8):
        @pl.when(jnp.logical_not((owner == me) & (other == head)))
        def _():
            copy(out_own.at[0], out_in.at[other], out_send.at[0], out_recv.at[other], me, head).wait_recv()
    for which, spot in ((0, far), (1, me)):
        for piece in range(4):
            n = 4 * which + piece
            where, token = spot // 2, (spot % 2) * 4 + piece
            mine = (where == me) & (token == head)

            @pl.when(jnp.logical_not(mine))
            def _():
                copy(out_own.at[n], out_in.at[head], out_send.at[n], out_recv.at[head], where, token).wait_send()

            @pl.when(mine)
            def _():
                pltpu.make_async_copy(out_own.at[n], out_in.at[head], out_local).wait()

    for pair in range(4):
        one = out_in[2 * pair].astype(jnp.float32)
        two = out_in[2 * pair + 1].astype(jnp.float32)
        one = jnp.concatenate([one[:, :HEAD_DIM], one[:, HEAD_DIM:]], axis=0)
        two = jnp.concatenate([two[:, :HEAD_DIM], two[:, HEAD_DIM:]], axis=0)
        out_ref[:, pl.ds(pair * 128, 128)] = jnp.concatenate([one, two], axis=1).astype(jnp.bfloat16)


def attention(queries, key_heads, value_heads, head_gain):
    rows = queries.shape[0]
    half = rows // 2
    return pl.pallas_call(
        attention_kernel,
        out_shape=jax.ShapeDtypeStruct((128, 8 * HEAD_DIM), jnp.bfloat16),
        in_specs=[pl.BlockSpec(memory_space=pltpu.VMEM)] * 4,
        out_specs=pl.BlockSpec(memory_space=pltpu.VMEM),
        scratch_shapes=[
            pltpu.VMEM((2, half, 128), jnp.bfloat16),
            pltpu.VMEM((2, half, 128), jnp.bfloat16),
            pltpu.VMEM((16, half, 128), jnp.bfloat16),
            pltpu.VMEM((16, half, 128), jnp.bfloat16),
            pltpu.VMEM((2, 16, half, 128), jnp.float32),
            pltpu.VMEM((2, 16, half, 128), jnp.float32),
            pltpu.VMEM((half, 128), jnp.float32),
            pltpu.VMEM((half, 128), jnp.float32),
            pltpu.VMEM((TILE, TILE), jnp.bfloat16),
            pltpu.VMEM((8, 64, 128), jnp.bfloat16),
            pltpu.VMEM((8, 64, 128), jnp.bfloat16),
            pltpu.SemaphoreType.DMA((2,)),
            pltpu.SemaphoreType.DMA((2,)),
            pltpu.SemaphoreType.DMA,
            pltpu.SemaphoreType.DMA((30,)),
            pltpu.SemaphoreType.DMA((16,)),
            pltpu.SemaphoreType.DMA((16,)),
            pltpu.SemaphoreType.DMA((8,)),
            pltpu.SemaphoreType.DMA((8,)),
            pltpu.SemaphoreType.DMA,
        ],
        compiler_params=pltpu.CompilerParams(vmem_limit_bytes=40 << 20, has_side_effects=True),
        name="attention",
    )(queries, key_heads, value_heads, head_gain.reshape(1, HEAD_DIM))


def mixture_kernel(
    head_ref, residual_ref, gain_ref, expert_ref, route_ref,
    out_weight, shared_gate, shared_up, shared_down, expert_gate, expert_up, expert_down,
    final_ref,
    ow_ref, sg_ref, su_ref, sd_ref, eg_ref, eu_ref, ed_ref,
    stream_ref, x_ref, place_ref, mix_ref, stage_ref, outgoing, arrived, rows_ref, hidden_ref,
    result, returned, total_ref,
    load_sem, out_send, out_recv, back_send, back_recv, local_sem,
):
    me = lax.axis_index("sp") * 8 + lax.axis_index("tp")
    tokens, width = residual_ref.shape
    devices, slots = 128, 3
    chunks = width // 128
    hidden = sg_ref.shape[1]
    f32, bf16 = jnp.float32, jnp.bfloat16

    loads = [
        pltpu.make_async_copy(source, target, load_sem.at[n])
        for n, (source, target) in enumerate(
            (
                (out_weight, ow_ref), (shared_gate, sg_ref), (shared_up, su_ref), (shared_down, sd_ref),
                (expert_gate, eg_ref), (expert_up, eu_ref), (expert_down, ed_ref),
            )
        )
    ]
    for one in loads:
        one.start()

    line = lax.broadcasted_iota(jnp.int32, (2 * devices, tokens), 0)
    expert = 2 * (line % devices) + line // devices
    named = jnp.zeros((2 * devices, tokens), f32)
    weight = jnp.zeros((2 * devices, tokens), f32)
    for pick in range(expert_ref.shape[0]):
        hit = expert_ref[pick : pick + 1, :] == expert
        named = named + jnp.where(hit, 1.0, 0.0)
        weight = weight + jnp.where(hit, route_ref[pick : pick + 1, :], 0.0)
    before = lax.broadcasted_iota(jnp.int32, (tokens, tokens), 0) < lax.broadcasted_iota(
        jnp.int32, (tokens, tokens), 1
    )
    rank = jnp.dot(
        named.astype(bf16), jnp.where(before, 1.0, 0.0).astype(bf16), preferred_element_type=f32
    )
    for slot in range(slots):
        chosen = jnp.where(rank == float(slot), named, 0.0)
        for side in range(2):
            part = chosen[side * devices : (side + 1) * devices]
            place_ref[side, slot] = part.astype(bf16)
            mix = (part * weight[side * devices : (side + 1) * devices]).T
            high = mix.astype(bf16)
            mix_ref[0, side, slot] = high
            mix_ref[1, side, slot] = (mix - high.astype(f32)).astype(bf16)

    loads[0].wait()
    squares = jnp.zeros((tokens, 1), f32)
    for n in range(width // 512):
        at = pl.ds(n * 512, 512)
        branch = jnp.dot(head_ref[...], ow_ref[:, at], preferred_element_type=f32)
        stream = (residual_ref[:, at].astype(f32) + branch).astype(bf16).astype(f32)
        stream_ref[:, at] = stream
        squares = squares + jnp.sum(stream * stream, axis=1, keepdims=True)
    inverse = lax.rsqrt(squares / width + EPSILON)
    for n in range(width // 512):
        at = pl.ds(n * 512, 512)
        x_ref[:, at] = (stream_ref[:, at] * inverse * gain_ref[:, at]).astype(bf16)

    def copy(source, target, send, receive, where):
        return pltpu.make_async_remote_copy(
            src_ref=source, dst_ref=target, send_sem=send, recv_sem=receive,
            device_id=(where // 8, where % 8), device_id_type=MESH,
        )

    def stage_to(target, side):
        def one(n, unused):
            block = stage_ref[pl.ds(n * 384, 384), :].astype(bf16)
            for k in range(8):
                target[side, n * 8 + k] = block[k * 48 : (k + 1) * 48]
            return unused

        lax.fori_loop(0, devices // 8, one, 0)

    def stage_from(source, side):
        def one(n, unused):
            for k in range(8):
                at = n * 384 + k * 48
                stage_ref[pl.ds(at, 48), :] = source[side, n * 8 + k].astype(f32)
            return unused

        lax.fori_loop(0, devices // 8, one, 0)

    def exchange(source, target, send, receive, side):
        def one(n, unused):
            where = (me + n) % devices
            copy(source.at[side, where], target.at[side, me], send.at[side], receive.at[side], where).start()
            return unused

        lax.fori_loop(1, devices, one, 0)
        pltpu.make_async_copy(source.at[side, me], target.at[side, me], local_sem).start()
        pltpu.make_async_copy(source.at[side, me], target.at[side, me], local_sem).wait()

    def wait_all(buffer, sem, side):
        everyone = buffer.at[side, pl.ds(0, devices - 1)]
        pltpu.make_async_copy(everyone, everyone, sem.at[side]).wait()

    for side in range(2):
        for slot in range(slots):
            place = place_ref[side, slot]

            def gather(n, unused):
                at = pl.multiple_of(n * 512, 512)
                rows = jnp.dot(place, x_ref[:, pl.ds(at, 512)], preferred_element_type=f32)
                for k in range(4):
                    stage_ref[pl.ds(slot * chunks + n * 4 + k, devices, stride=slots * chunks), :] = (
                        rows[:, k * 128 : (k + 1) * 128]
                    )
                return unused

            lax.fori_loop(0, width // 512, gather, 0)
        stage_to(outgoing, side)
        exchange(outgoing, arrived, out_send, out_recv, side)

    for one in loads[1:4]:
        one.wait()
    gate = jnp.dot(x_ref[...], sg_ref[...], preferred_element_type=f32)
    up = jnp.dot(x_ref[...], su_ref[...], preferred_element_type=f32)
    shared = (gate / (1.0 + jnp.exp(-gate)) * up).astype(bf16)
    for n in range(width // 512):
        at = pl.ds(n * 512, 512)
        total_ref[:, at] = stream_ref[:, at] + jnp.dot(
            shared, sd_ref[:, at], preferred_element_type=f32
        )
    for one in loads[4:]:
        one.wait()

    count = devices * slots
    for side in range(2):
        wait_all(arrived, out_recv, side)
        stage_from(arrived, side)
        for k in range(chunks):
            rows_ref[:, pl.ds(k * 128, 128)] = stage_ref[pl.ds(k, count, stride=chunks), :].astype(bf16)

        def inner(n, unused):
            at = pl.ds(pl.multiple_of(n * 256, 256), 256)
            gate = jnp.dot(rows_ref[...], eg_ref[side, :, at], preferred_element_type=f32)
            up = jnp.dot(rows_ref[...], eu_ref[side, :, at], preferred_element_type=f32)
            hidden_ref[:, at] = (gate / (1.0 + jnp.exp(-gate)) * up).astype(bf16)
            return unused

        lax.fori_loop(0, hidden // 256, inner, 0)

        def outer(n, unused):
            at = pl.ds(pl.multiple_of(n * 256, 256), 256)
            rows = jnp.dot(hidden_ref[...], ed_ref[side, :, at], preferred_element_type=f32)
            for k in range(2):
                stage_ref[pl.ds(n * 2 + k, count, stride=chunks), :] = rows[:, k * 128 : (k + 1) * 128]
            return unused

        lax.fori_loop(0, width // 256, outer, 0)
        stage_to(result, side)
        exchange(result, returned, back_send, back_recv, side)

    for side in range(2):
        wait_all(returned, back_recv, side)
        stage_from(returned, side)
        for k in range(chunks):
            at = pl.ds(k * 128, 128)
            total = total_ref[:, at]
            for slot in range(slots):
                rows = stage_ref[pl.ds(slot * chunks + k, devices, stride=slots * chunks), :].astype(bf16)
                for level in range(2):
                    total = total + jnp.dot(
                        mix_ref[level, side, slot], rows, preferred_element_type=f32
                    )
            total_ref[:, at] = total
    final_ref[...] = total_ref[...].astype(bf16)
    for side in range(2):
        wait_all(outgoing, out_send, side)
        wait_all(result, back_send, side)


def mixture(
    heads, residual, out_weight, norm_gain, shared_gate, shared_up, shared_down,
    expert_gate, expert_up, expert_down, routed_experts, route_weights,
):
    tokens, width = residual.shape
    hidden = shared_gate.shape[1]
    bf16, f32 = jnp.bfloat16, jnp.float32
    vmem, anywhere = pl.BlockSpec(memory_space=pltpu.VMEM), pl.BlockSpec(memory_space=pl.ANY)
    blocks = (2, 128, 48, 128)
    return pl.pallas_call(
        mixture_kernel,
        out_shape=jax.ShapeDtypeStruct((tokens, width), bf16),
        in_specs=[vmem] * 5 + [anywhere] * 7,
        out_specs=vmem,
        scratch_shapes=[
            pltpu.VMEM(out_weight.shape, bf16),
            pltpu.VMEM(shared_gate.shape, bf16),
            pltpu.VMEM(shared_up.shape, bf16),
            pltpu.VMEM(shared_down.shape, bf16),
            pltpu.VMEM(expert_gate.shape, bf16),
            pltpu.VMEM(expert_up.shape, bf16),
            pltpu.VMEM(expert_down.shape, bf16),
            pltpu.VMEM((tokens, width), f32),
            pltpu.VMEM((tokens, width), bf16),
            pltpu.VMEM((2, 3, 128, tokens), bf16),
            pltpu.VMEM((2, 2, 3, tokens, 128), bf16),
            pltpu.VMEM((128 * 48, 128), f32),
            pltpu.VMEM(blocks, bf16),
            pltpu.VMEM(blocks, bf16),
            pltpu.VMEM((384, width), bf16),
            pltpu.VMEM((384, hidden), bf16),
            pltpu.VMEM(blocks, bf16),
            pltpu.VMEM(blocks, bf16),
            pltpu.VMEM((tokens, width), f32),
            pltpu.SemaphoreType.DMA((7,)),
            pltpu.SemaphoreType.DMA((2,)),
            pltpu.SemaphoreType.DMA((2,)),
            pltpu.SemaphoreType.DMA((2,)),
            pltpu.SemaphoreType.DMA((2,)),
            pltpu.SemaphoreType.DMA,
        ],
        compiler_params=pltpu.CompilerParams(vmem_limit_bytes=60 << 20, has_side_effects=True),
        name="mixture",
    )(
        heads, residual, norm_gain.reshape(1, width), routed_experts.T, route_weights.T,
        out_weight, shared_gate, shared_up, shared_down, expert_gate, expert_up, expert_down,
    )


def body(
    queries,
    key_heads,
    value_heads,
    head_gain,
    residual,
    out_weight,
    norm_gain,
    shared_gate,
    shared_up,
    shared_down,
    expert_gate,
    expert_up,
    expert_down,
    routed_experts,
    route_weights,
):
    heads = attention(queries, key_heads, value_heads, head_gain)
    return mixture(
        heads,
        residual,
        out_weight,
        norm_gain,
        shared_gate,
        shared_up,
        shared_down,
        expert_gate,
        expert_up,
        expert_down,
        routed_experts,
        route_weights,
    )


def solution(mesh):
    return jax.shard_map(
        body,
        mesh=mesh,
        in_specs=(
            P("sp", "tp"),
            P("sp", "tp"),
            P("sp", "tp"),
            P("tp"),
            P(("sp", "tp"), None),
            P(),
            P(),
            P(),
            P(),
            P(),
            P(("sp", "tp"), None, None),
            P(("sp", "tp"), None, None),
            P(("sp", "tp"), None, None),
            P(("sp", "tp"), None),
            P(("sp", "tp"), None),
        ),
        out_specs=P(("sp", "tp"), None),
        check_vma=False,
    )
```

```python
import math

import jax
import jax.numpy as jnp
from jax import lax
from jax.experimental import pallas as pl
from jax.experimental.pallas import tpu as pltpu
from jax.sharding import PartitionSpec as P

HEAD_DIM = 64


EPSILON = 1e-06


LOG2E = 1.4426950408889634
TILE = 256
MESH = pl.DeviceIdType.MESH


def tile_terms(q2, keys, values, tri, carry, mask):
    x = jnp.dot(q2, keys, preferred_element_type=jnp.float32)
    x = jnp.minimum(x, 126.0)
    drop = jnp.log(1.0 + jnp.exp2(x)) * LOG2E
    stick = x - drop
    if mask is not None:
        drop = jnp.where(mask, drop, 0.0)
    after = jnp.dot(drop.astype(jnp.bfloat16), tri, preferred_element_type=jnp.float32)
    both = jnp.concatenate([carry, carry], axis=1)
    weights = jnp.exp2(stick - after - both)
    if mask is not None:
        weights = jnp.where(mask, weights, 0.0)
    out = jnp.dot(weights.astype(jnp.bfloat16), values, preferred_element_type=jnp.float32)
    total = after[:, :1] + drop[:, :1]
    return out, carry + jnp.broadcast_to(total, carry.shape)


def attention_kernel(
    q_ref, k_ref, v_ref, gain_ref, out_ref,
    q_own, q_ref2, key_ref, value_ref, acc_ref, carry_ref, sum_ref, past_ref, tri_ref, out_own, out_in,
    q_send, q_recv, send_sem, key_recv, value_recv, out_send, out_recv, out_local,
):
    me, head = lax.axis_index("sp"), lax.axis_index("tp")
    row, column = me // 4, me % 4
    half = q_ref.shape[0] // 2

    q = q_ref[...].astype(jnp.float32) * (LOG2E / math.sqrt(HEAD_DIM))
    high = q.astype(jnp.bfloat16)
    low = (q - high.astype(jnp.float32)).astype(jnp.bfloat16)
    both = jnp.concatenate([high, low], axis=1)
    q_ref2[0] = both[:half]
    q_own[...] = both[half:]
    for part in range(8):
        block = k_ref[pl.ds(part * 128, 128), :].astype(jnp.float32)
        key_ref[me, pl.ds(part * HEAD_DIM, HEAD_DIM), :] = block.T.astype(jnp.bfloat16)
    v = v_ref[...].astype(jnp.float32)
    value_ref[me] = jnp.concatenate([v[:half], v[half:]], axis=1).astype(jnp.bfloat16)

    def copy(source, target, out_sem, in_sem, where, which):
        return pltpu.make_async_remote_copy(
            src_ref=source, dst_ref=target, send_sem=out_sem, recv_sem=in_sem,
            device_id=(where, which), device_id_type=MESH,
        )

    q_copy = copy(q_own, q_ref2.at[1], q_send, q_recv, 15 - me, head)
    q_copy.start()
    steps = (1, 3, 2)

    def key_copy(block, n, where):
        return copy(key_ref.at[block], key_ref.at[block], send_sem.at[n], key_recv.at[block], where, head)

    def value_copy(block, n, where):
        return copy(value_ref.at[block], value_ref.at[block], send_sem.at[n], value_recv.at[block], where, head)

    along = [row * 4 + (column + d) % 4 for d in steps]
    across = [(row + d) % 4 * 4 + column for d in steps]
    sent = []
    for n in range(3):
        sent.append(key_copy(me, n, along[n]))
        sent.append(value_copy(me, 3 + n, across[n]))
    for n in range(3):
        sent.append(key_copy(me, 6 + n, across[n]))
        sent.append(value_copy(me, 9 + n, along[n]))
    for one in sent:
        one.start()

    r = lax.broadcasted_iota(jnp.int32, (TILE, TILE), 0)
    c = lax.broadcasted_iota(jnp.int32, (TILE, TILE), 1)
    tri_ref[...] = (r > c).astype(jnp.float32).astype(jnp.bfloat16)
    passed = []

    def forward():
        for n in range(3):
            key_copy(along[n], 0, me).wait_recv()
            for m in range(3):
                key_copy(along[n], 12 + 3 * n + m, across[m]).start()
            value_copy(across[n], 0, me).wait_recv()
            for m in range(3):
                value_copy(across[n], 21 + 3 * n + m, along[m]).start()

    for n in range(3):
        for m in range(3):
            passed.append(key_copy(along[n], 12 + 3 * n + m, across[m]))
            passed.append(value_copy(across[n], 21 + 3 * n + m, along[m]))

    def arrived(block):
        @pl.when(block // 4 != row)
        def _():
            key_copy(block, 0, me).wait_recv()

        @pl.when(block % 4 != column)
        def _():
            value_copy(block, 0, me).wait_recv()

    def unit(which, place, diagonal):
        block, side = place // 2, place % 2
        for part in (1, 0):
            at = (2 * side + part) * 128
            left = key_ref[block, pl.ds(at, HEAD_DIM), :]
            right = key_ref[block, pl.ds(at + HEAD_DIM, HEAD_DIM), :]
            keys = jnp.concatenate([left, right], axis=1)
            keys = jnp.concatenate([keys, keys], axis=0)
            values = value_ref[block, pl.ds(part * TILE, TILE), :]
            lanes = lax.broadcasted_iota(jnp.int32, values.shape, 1) // HEAD_DIM
            values = jnp.where(lanes == side, values, jnp.zeros_like(values))
            rows, mask = pl.ds(0, half), None
            if diagonal and part == 1:
                rows, mask = pl.ds(TILE, TILE), c < r
            elif diagonal:
                mask = lax.broadcasted_iota(jnp.int32, (half, TILE), 1) < lax.broadcasted_iota(
                    jnp.int32, (half, TILE), 0
                )
            out, carry = tile_terms(
                q_ref2[which, rows, :], keys, values, tri_ref[...], carry_ref[which, block, rows, :], mask
            )
            acc_ref[which, block, rows, :] += out
            carry_ref[which, block, rows, :] = carry

    def finish(which, place):
        blank = jnp.zeros((half, 128), jnp.float32)
        sum_ref[...] = blank
        past_ref[...] = blank

        def later(n, unused):
            block = place // 2 - n
            sum_ref[...] += jnp.exp2(-past_ref[...]) * acc_ref[which, block]
            past_ref[...] += carry_ref[which, block]
            return unused

        lax.fori_loop(0, place // 2 + 1, later, 0)
        acc = sum_ref[...]
        mixed = acc[:, :HEAD_DIM] + acc[:, HEAD_DIM:]
        inverse = lax.rsqrt(jnp.mean(mixed * mixed, axis=1, keepdims=True) + EPSILON)
        normed = mixed * inverse * gain_ref[...]
        for piece in range(4):
            at = piece * 128
            two = jnp.concatenate([normed[at : at + 64], normed[at + 64 : at + 128]], axis=1)
            out_own[4 * which + piece] = two.astype(jnp.bfloat16)
        for piece in range(4):
            n = 4 * which + piece
            where, token = place // 2, (place % 2) * 4 + piece
            mine = (where == me) & (token == head)

            @pl.when(jnp.logical_not(mine))
            def _():
                copy(out_own.at[n], out_in.at[head], out_send.at[n], out_recv.at[head], where, token).start()

            @pl.when(mine)
            def _():
                pltpu.make_async_copy(out_own.at[n], out_in.at[head], out_local).start()

    far = jnp.maximum(2 * me, 31 - 2 * me)
    order = ((0, 0), (0, 1), (1, 0), (0, 3), (3, 0), (0, 2), (2, 0), (1, 1), (3, 3), (1, 3), (3, 1), (1, 2), (2, 1), (3, 2), (2, 3), (2, 2))

    def pick(n, axis):
        return sum(jnp.where(n == k, one[axis], 0) for k, one in enumerate(order))

    def visit(n, unused):
        block = (row + pick(n, 0)) % 4 * 4 + (column + pick(n, 1)) % 4

        @pl.when(n == 1)
        def _():
            forward()

        @pl.when((block <= far // 2) & (n > 0))
        def _():
            arrived(block)

        def pair(i, unused):
            which, side = i // 2, 1 - i % 2
            top = jnp.where(which == 0, 2 * me, 31 - 2 * me)
            place = 2 * block + side

            @pl.when((n == 0) & (i == 2))
            def _():
                q_copy.wait_recv()

            @pl.when((side == 1) & (2 * block <= top))
            def _():
                acc_ref[which, block] = jnp.zeros((half, 128), jnp.float32)
                carry_ref[which, block] = jnp.zeros((half, 128), jnp.float32)

            @pl.when(place < top)
            def _():
                unit(which, place, False)

            @pl.when(place == top)
            def _():
                unit(which, place, True)

            return unused

        @pl.when(block <= far // 2)
        def _():
            lax.fori_loop(0, 4, pair, 0)

        return unused

    lax.fori_loop(0, 16, visit, 0)
    finish(0, 2 * me)
    finish(1, 31 - 2 * me)

    def drain(n, unused):
        @pl.when(n != me)
        def _():
            arrived(n)

        return unused

    lax.fori_loop(far // 2 + 1, 16, drain, 0)
    q_copy.wait_send()
    for one in sent + passed:
        one.wait_send()

    for other in range(8):
        @pl.when(jnp.logical_not((head < 4) & (other == head)))
        def _():
            copy(out_own.at[0], out_in.at[other], out_send.at[0], out_recv.at[other], me, head).wait_recv()
    for which, spot in ((0, 2 * me), (1, 31 - 2 * me)):
        for piece in range(4):
            n = 4 * which + piece
            where, token = spot // 2, (spot % 2) * 4 + piece
            mine = (where == me) & (token == head)

            @pl.when(jnp.logical_not(mine))
            def _():
                copy(out_own.at[n], out_in.at[head], out_send.at[n], out_recv.at[head], where, token).wait_send()

            @pl.when(mine)
            def _():
                pltpu.make_async_copy(out_own.at[n], out_in.at[head], out_local).wait()

    for pair in range(4):
        one = out_in[2 * pair].astype(jnp.float32)
        two = out_in[2 * pair + 1].astype(jnp.float32)
        one = jnp.concatenate([one[:, :HEAD_DIM], one[:, HEAD_DIM:]], axis=0)
        two = jnp.concatenate([two[:, :HEAD_DIM], two[:, HEAD_DIM:]], axis=0)
        out_ref[:, pl.ds(pair * 128, 128)] = jnp.concatenate([one, two], axis=1).astype(jnp.bfloat16)


def attention(queries, key_heads, value_heads, head_gain):
    rows = queries.shape[0]
    half = rows // 2
    return pl.pallas_call(
        attention_kernel,
        out_shape=jax.ShapeDtypeStruct((128, 8 * HEAD_DIM), jnp.bfloat16),
        in_specs=[pl.BlockSpec(memory_space=pltpu.VMEM)] * 4,
        out_specs=pl.BlockSpec(memory_space=pltpu.VMEM),
        scratch_shapes=[
            pltpu.VMEM((half, 128), jnp.bfloat16),
            pltpu.VMEM((2, half, 128), jnp.bfloat16),
            pltpu.VMEM((16, half, 128), jnp.bfloat16),
            pltpu.VMEM((16, half, 128), jnp.bfloat16),
            pltpu.VMEM((2, 16, half, 128), jnp.float32),
            pltpu.VMEM((2, 16, half, 128), jnp.float32),
            pltpu.VMEM((half, 128), jnp.float32),
            pltpu.VMEM((half, 128), jnp.float32),
            pltpu.VMEM((TILE, TILE), jnp.bfloat16),
            pltpu.VMEM((8, 64, 128), jnp.bfloat16),
            pltpu.VMEM((8, 64, 128), jnp.bfloat16),
            pltpu.SemaphoreType.DMA,
            pltpu.SemaphoreType.DMA,
            pltpu.SemaphoreType.DMA((30,)),
            pltpu.SemaphoreType.DMA((16,)),
            pltpu.SemaphoreType.DMA((16,)),
            pltpu.SemaphoreType.DMA((8,)),
            pltpu.SemaphoreType.DMA((8,)),
            pltpu.SemaphoreType.DMA,
        ],
        compiler_params=pltpu.CompilerParams(vmem_limit_bytes=40 << 20, has_side_effects=True),
        name="attention",
    )(queries, key_heads, value_heads, head_gain.reshape(1, HEAD_DIM))


def mixture_kernel(
    head_ref, residual_ref, gain_ref, expert_ref, route_ref,
    out_weight, shared_gate, shared_up, shared_down, expert_gate, expert_up, expert_down,
    final_ref,
    ow_ref, sg_ref, su_ref, sd_ref, eg_ref, eu_ref, ed_ref,
    stream_ref, x_ref, place_ref, mix_ref, stage_ref, outgoing, arrived, rows_ref, hidden_ref,
    result, returned, total_ref,
    load_sem, out_send, out_recv, back_send, back_recv, local_sem,
):
    me = lax.axis_index("sp") * 8 + lax.axis_index("tp")
    tokens, width = residual_ref.shape
    devices, slots = 128, 3
    chunks = width // 128
    hidden = sg_ref.shape[1]
    f32, bf16 = jnp.float32, jnp.bfloat16

    loads = [
        pltpu.make_async_copy(source, target, load_sem.at[n])
        for n, (source, target) in enumerate(
            (
                (out_weight, ow_ref), (shared_gate, sg_ref), (shared_up, su_ref), (shared_down, sd_ref),
                (expert_gate, eg_ref), (expert_up, eu_ref), (expert_down, ed_ref),
            )
        )
    ]
    for one in loads:
        one.start()

    line = lax.broadcasted_iota(jnp.int32, (2 * devices, tokens), 0)
    expert = 2 * (line % devices) + line // devices
    named = jnp.zeros((2 * devices, tokens), f32)
    weight = jnp.zeros((2 * devices, tokens), f32)
    for pick in range(expert_ref.shape[0]):
        hit = expert_ref[pick : pick + 1, :] == expert
        named = named + jnp.where(hit, 1.0, 0.0)
        weight = weight + jnp.where(hit, route_ref[pick : pick + 1, :], 0.0)
    before = lax.broadcasted_iota(jnp.int32, (tokens, tokens), 0) < lax.broadcasted_iota(
        jnp.int32, (tokens, tokens), 1
    )
    rank = jnp.dot(
        named.astype(bf16), jnp.where(before, 1.0, 0.0).astype(bf16), preferred_element_type=f32
    )
    for slot in range(slots):
        chosen = jnp.where(rank == float(slot), named, 0.0)
        for side in range(2):
            part = chosen[side * devices : (side + 1) * devices]
            place_ref[side, slot] = part.astype(bf16)
            mix = (part * weight[side * devices : (side + 1) * devices]).T
            high = mix.astype(bf16)
            mix_ref[0, side, slot] = high
            mix_ref[1, side, slot] = (mix - high.astype(f32)).astype(bf16)

    loads[0].wait()
    squares = jnp.zeros((tokens, 1), f32)
    for n in range(width // 512):
        at = pl.ds(n * 512, 512)
        branch = jnp.dot(head_ref[...], ow_ref[:, at], preferred_element_type=f32)
        stream = (residual_ref[:, at].astype(f32) + branch).astype(bf16).astype(f32)
        stream_ref[:, at] = stream
        squares = squares + jnp.sum(stream * stream, axis=1, keepdims=True)
    inverse = lax.rsqrt(squares / width + EPSILON)
    for n in range(width // 512):
        at = pl.ds(n * 512, 512)
        x_ref[:, at] = (stream_ref[:, at] * inverse * gain_ref[:, at]).astype(bf16)

    def copy(source, target, send, receive, where):
        return pltpu.make_async_remote_copy(
            src_ref=source, dst_ref=target, send_sem=send, recv_sem=receive,
            device_id=(where // 8, where % 8), device_id_type=MESH,
        )

    def stage_to(target, side):
        def one(n, unused):
            block = stage_ref[pl.ds(n * 384, 384), :].astype(bf16)
            for k in range(8):
                target[side, n * 8 + k] = block[k * 48 : (k + 1) * 48]
            return unused

        lax.fori_loop(0, devices // 8, one, 0)

    def stage_from(source, side):
        def one(n, unused):
            for k in range(8):
                at = n * 384 + k * 48
                stage_ref[pl.ds(at, 48), :] = source[side, n * 8 + k].astype(f32)
            return unused

        lax.fori_loop(0, devices // 8, one, 0)

    def exchange(source, target, send, receive, side):
        def one(n, unused):
            where = (me + 37 * n) % devices
            copy(source.at[side, where], target.at[side, me], send.at[side], receive.at[side], where).start()
            return unused

        lax.fori_loop(1, devices, one, 0)
        pltpu.make_async_copy(source.at[side, me], target.at[side, me], local_sem).start()
        pltpu.make_async_copy(source.at[side, me], target.at[side, me], local_sem).wait()

    def wait_all(buffer, sem, side):
        everyone = buffer.at[side, pl.ds(0, devices - 1)]
        pltpu.make_async_copy(everyone, everyone, sem.at[side]).wait()

    for side in range(2):
        for slot in range(slots):
            place = place_ref[side, slot]

            def gather(n, unused):
                at = pl.multiple_of(n * 512, 512)
                rows = jnp.dot(place, x_ref[:, pl.ds(at, 512)], preferred_element_type=f32)
                for k in range(4):
                    stage_ref[pl.ds(slot * chunks + n * 4 + k, devices, stride=slots * chunks), :] = (
                        rows[:, k * 128 : (k + 1) * 128]
                    )
                return unused

            lax.fori_loop(0, width // 512, gather, 0)
        stage_to(outgoing, side)
        exchange(outgoing, arrived, out_send, out_recv, side)

    for one in loads[1:4]:
        one.wait()
    gate = jnp.dot(x_ref[...], sg_ref[...], preferred_element_type=f32)
    up = jnp.dot(x_ref[...], su_ref[...], preferred_element_type=f32)
    shared = (gate / (1.0 + jnp.exp(-gate)) * up).astype(bf16)
    for n in range(width // 512):
        at = pl.ds(n * 512, 512)
        total_ref[:, at] = stream_ref[:, at] + jnp.dot(
            shared, sd_ref[:, at], preferred_element_type=f32
        )
    for one in loads[4:]:
        one.wait()

    count = devices * slots
    for side in range(2):
        wait_all(arrived, out_recv, side)
        stage_from(arrived, side)
        for k in range(chunks):
            rows_ref[:, pl.ds(k * 128, 128)] = stage_ref[pl.ds(k, count, stride=chunks), :].astype(bf16)

        def inner(n, unused):
            at = pl.ds(pl.multiple_of(n * 256, 256), 256)
            gate = jnp.dot(rows_ref[...], eg_ref[side, :, at], preferred_element_type=f32)
            up = jnp.dot(rows_ref[...], eu_ref[side, :, at], preferred_element_type=f32)
            hidden_ref[:, at] = (gate / (1.0 + jnp.exp(-gate)) * up).astype(bf16)
            return unused

        lax.fori_loop(0, hidden // 256, inner, 0)

        def outer(n, unused):
            at = pl.ds(pl.multiple_of(n * 256, 256), 256)
            rows = jnp.dot(hidden_ref[...], ed_ref[side, :, at], preferred_element_type=f32)
            for k in range(2):
                stage_ref[pl.ds(n * 2 + k, count, stride=chunks), :] = rows[:, k * 128 : (k + 1) * 128]
            return unused

        lax.fori_loop(0, width // 256, outer, 0)
        stage_to(result, side)
        exchange(result, returned, back_send, back_recv, side)

    for side in range(2):
        wait_all(returned, back_recv, side)
        stage_from(returned, side)
        for k in range(chunks):
            at = pl.ds(k * 128, 128)
            total = total_ref[:, at]
            for slot in range(slots):
                rows = stage_ref[pl.ds(slot * chunks + k, devices, stride=slots * chunks), :].astype(bf16)
                for level in range(2):
                    total = total + jnp.dot(
                        mix_ref[level, side, slot], rows, preferred_element_type=f32
                    )
            total_ref[:, at] = total
    final_ref[...] = total_ref[...].astype(bf16)
    for side in range(2):
        wait_all(outgoing, out_send, side)
        wait_all(result, back_send, side)


def mixture(
    heads, residual, out_weight, norm_gain, shared_gate, shared_up, shared_down,
    expert_gate, expert_up, expert_down, routed_experts, route_weights,
):
    tokens, width = residual.shape
    hidden = shared_gate.shape[1]
    bf16, f32 = jnp.bfloat16, jnp.float32
    vmem, anywhere = pl.BlockSpec(memory_space=pltpu.VMEM), pl.BlockSpec(memory_space=pl.ANY)
    blocks = (2, 128, 48, 128)
    return pl.pallas_call(
        mixture_kernel,
        out_shape=jax.ShapeDtypeStruct((tokens, width), bf16),
        in_specs=[vmem] * 5 + [anywhere] * 7,
        out_specs=vmem,
        scratch_shapes=[
            pltpu.VMEM(out_weight.shape, bf16),
            pltpu.VMEM(shared_gate.shape, bf16),
            pltpu.VMEM(shared_up.shape, bf16),
            pltpu.VMEM(shared_down.shape, bf16),
            pltpu.VMEM(expert_gate.shape, bf16),
            pltpu.VMEM(expert_up.shape, bf16),
            pltpu.VMEM(expert_down.shape, bf16),
            pltpu.VMEM((tokens, width), f32),
            pltpu.VMEM((tokens, width), bf16),
            pltpu.VMEM((2, 3, 128, tokens), bf16),
            pltpu.VMEM((2, 2, 3, tokens, 128), bf16),
            pltpu.VMEM((128 * 48, 128), f32),
            pltpu.VMEM(blocks, bf16),
            pltpu.VMEM(blocks, bf16),
            pltpu.VMEM((384, width), bf16),
            pltpu.VMEM((384, hidden), bf16),
            pltpu.VMEM(blocks, bf16),
            pltpu.VMEM(blocks, bf16),
            pltpu.VMEM((tokens, width), f32),
            pltpu.SemaphoreType.DMA((7,)),
            pltpu.SemaphoreType.DMA((2,)),
            pltpu.SemaphoreType.DMA((2,)),
            pltpu.SemaphoreType.DMA((2,)),
            pltpu.SemaphoreType.DMA((2,)),
            pltpu.SemaphoreType.DMA,
        ],
        compiler_params=pltpu.CompilerParams(vmem_limit_bytes=60 << 20, has_side_effects=True),
        name="mixture",
    )(
        heads, residual, norm_gain.reshape(1, width), routed_experts.T, route_weights.T,
        out_weight, shared_gate, shared_up, shared_down, expert_gate, expert_up, expert_down,
    )


def body(
    queries,
    key_heads,
    value_heads,
    head_gain,
    residual,
    out_weight,
    norm_gain,
    shared_gate,
    shared_up,
    shared_down,
    expert_gate,
    expert_up,
    expert_down,
    routed_experts,
    route_weights,
):
    heads = attention(queries, key_heads, value_heads, head_gain)
    return mixture(
        heads,
        residual,
        out_weight,
        norm_gain,
        shared_gate,
        shared_up,
        shared_down,
        expert_gate,
        expert_up,
        expert_down,
        routed_experts,
        route_weights,
    )


def solution(mesh):
    return jax.shard_map(
        body,
        mesh=mesh,
        in_specs=(
            P("sp", "tp"),
            P("sp", "tp"),
            P("sp", "tp"),
            P("tp"),
            P(("sp", "tp"), None),
            P(),
            P(),
            P(),
            P(),
            P(),
            P(("sp", "tp"), None, None),
            P(("sp", "tp"), None, None),
            P(("sp", "tp"), None, None),
            P(("sp", "tp"), None),
            P(("sp", "tp"), None),
        ),
        out_specs=P(("sp", "tp"), None),
        check_vma=False,
    )
```

```python
import math

import jax
import jax.numpy as jnp
from jax import lax
from jax.experimental import pallas as pl
from jax.experimental.pallas import tpu as pltpu
from jax.sharding import PartitionSpec as P

HEAD_DIM = 64


EPSILON = 1e-06


LOG2E = 1.4426950408889634
TILE = 256
MESH = pl.DeviceIdType.MESH


def tile_terms(q2, keys, values, tri, carry, mask):
    x = jnp.dot(q2, keys, preferred_element_type=jnp.float32)
    x = jnp.minimum(x, 126.0)
    drop = jnp.log(1.0 + jnp.exp2(x)) * LOG2E
    stick = x - drop
    if mask is not None:
        drop = jnp.where(mask, drop, 0.0)
    after = jnp.dot(drop.astype(jnp.bfloat16), tri, preferred_element_type=jnp.float32)
    both = jnp.concatenate([carry, carry], axis=1)
    weights = jnp.exp2(stick - after - both)
    if mask is not None:
        weights = jnp.where(mask, weights, 0.0)
    out = jnp.dot(weights.astype(jnp.bfloat16), values, preferred_element_type=jnp.float32)
    total = after[:, :1] + drop[:, :1]
    return out, carry + jnp.broadcast_to(total, carry.shape)


def remote(source, target, send, receive, where):
    return pltpu.make_async_remote_copy(
        src_ref=source, dst_ref=target, send_sem=send, recv_sem=receive,
        device_id=where, device_id_type=MESH,
    )


def route(expert_ref, route_ref, place_ref, mix_ref):
    devices, slots, tokens = 128, 3, expert_ref.shape[1]
    f32, bf16 = jnp.float32, jnp.bfloat16
    line = lax.broadcasted_iota(jnp.int32, (2 * devices, tokens), 0)
    expert = 2 * (line % devices) + line // devices
    named = jnp.zeros((2 * devices, tokens), f32)
    weight = jnp.zeros((2 * devices, tokens), f32)
    for pick in range(expert_ref.shape[0]):
        hit = expert_ref[pick : pick + 1, :] == expert
        named = named + jnp.where(hit, 1.0, 0.0)
        if mix_ref is not None:
            weight = weight + jnp.where(hit, route_ref[pick : pick + 1, :], 0.0)
    before = lax.broadcasted_iota(jnp.int32, (tokens, tokens), 0) < lax.broadcasted_iota(
        jnp.int32, (tokens, tokens), 1
    )
    rank = jnp.dot(
        named.astype(bf16), jnp.where(before, 1.0, 0.0).astype(bf16), preferred_element_type=f32
    )
    for slot in range(slots):
        chosen = jnp.where(rank == float(slot), named, 0.0)
        for side in range(2):
            part = chosen[side * devices : (side + 1) * devices]
            place_ref[side, slot] = part.astype(bf16)
            if mix_ref is not None:
                mix = (part * weight[side * devices : (side + 1) * devices]).T
                high = mix.astype(bf16)
                mix_ref[0, side, slot] = high
                mix_ref[1, side, slot] = (mix - high.astype(f32)).astype(bf16)


def collect(place_ref, side, from_ref, stage_ref, outgoing):
    for slot in range(3):
        place = place_ref[side, slot]

        def gather(n, unused):
            at = pl.multiple_of(n * 512, 512)
            rows = jnp.dot(place, from_ref[:, pl.ds(at, 512)], preferred_element_type=jnp.float32)
            for k in range(4):
                stage_ref[pl.ds(slot * 16 + n * 4 + k, 128, stride=48), :] = (
                    rows[:, k * 128 : (k + 1) * 128]
                )
            return unused

        lax.fori_loop(0, from_ref.shape[1] // 512, gather, 0)

    def move(n, unused):
        block = stage_ref[pl.ds(n * 384, 384), :].astype(jnp.bfloat16)
        for k in range(8):
            outgoing[n * 8 + k] = block[k * 48 : (k + 1) * 48]
        return unused

    lax.fori_loop(0, 16, move, 0)


def spread(source, target, send, receive, own, me):
    def go(n):
        where = lax.rem(me + 37 * n, 128)
        device = (lax.div(where, 8), lax.rem(where, 8))
        remote(source.at[where], target.at[me], send, receive, device).start()

    def several(n, unused):
        for k in range(7):
            go(7 * n + k + 1)
        return unused

    lax.fori_loop(0, 18, several, 0)
    go(127)
    pltpu.make_async_copy(source.at[me], target.at[me], own).start()


def spread_own(source, target, own, me):
    pltpu.make_async_copy(source.at[me], target.at[me], own).wait()


def spread_wait(buffer, sem):
    everyone = buffer.at[pl.ds(0, 127)]
    pltpu.make_async_copy(everyone, everyone, sem).wait()


def attention_kernel(
    q_ref, k_ref, v_ref, gain_ref, residual_ref, expert_ref, out_ref, arrived_ref,
    q_own, q_ref2, key_ref, value_ref, acc_ref, carry_ref, sum_ref, past_ref, tri_ref, out_own, out_in,
    place_ref, stage_ref, outgoing,
    q_send, q_recv, send_sem, key_recv, value_recv, out_send, out_recv, out_local,
    row_send, row_recv, row_local,
):
    me, head = lax.axis_index("sp"), lax.axis_index("tp")
    row, column = me // 4, me % 4
    half = q_ref.shape[1] // 2

    q = q_ref[...].astype(jnp.float32).T * (LOG2E / math.sqrt(HEAD_DIM))
    high = q.astype(jnp.bfloat16)
    low = (q - high.astype(jnp.float32)).astype(jnp.bfloat16)
    both = jnp.concatenate([high, low], axis=1)
    q_ref2[0] = both[:half]
    q_own[...] = both[half:]
    for part in range(8):
        key_ref[me, pl.ds(part * HEAD_DIM, HEAD_DIM), :] = k_ref[:, pl.ds(part * 128, 128)]
    v = v_ref[...].astype(jnp.float32).T
    value_ref[me] = jnp.concatenate([v[:half], v[half:]], axis=1).astype(jnp.bfloat16)

    def copy(source, target, out_sem, in_sem, where, which):
        return pltpu.make_async_remote_copy(
            src_ref=source, dst_ref=target, send_sem=out_sem, recv_sem=in_sem,
            device_id=(where, which), device_id_type=MESH,
        )

    q_copy = copy(q_own, q_ref2.at[1], q_send, q_recv, 15 - me, head)
    q_copy.start()
    steps = (1, 3, 2)

    def key_copy(block, n, where):
        return copy(key_ref.at[block], key_ref.at[block], send_sem.at[n], key_recv.at[block], where, head)

    def value_copy(block, n, where):
        return copy(value_ref.at[block], value_ref.at[block], send_sem.at[n], value_recv.at[block], where, head)

    along = [row * 4 + (column + d) % 4 for d in steps]
    across = [(row + d) % 4 * 4 + column for d in steps]
    sent = []
    for n in range(3):
        sent.append(key_copy(me, n, along[n]))
        sent.append(value_copy(me, 3 + n, across[n]))
    for n in range(3):
        sent.append(key_copy(me, 6 + n, across[n]))
        sent.append(value_copy(me, 9 + n, along[n]))
    for one in sent:
        one.start()

    r = lax.broadcasted_iota(jnp.int32, (TILE, TILE), 0)
    c = lax.broadcasted_iota(jnp.int32, (TILE, TILE), 1)
    tri_ref[...] = (r > c).astype(jnp.float32).astype(jnp.bfloat16)
    route(expert_ref, None, place_ref, None)
    collect(place_ref, 0, residual_ref, stage_ref, outgoing)

    passed = []

    def forward():
        for n in range(3):
            key_copy(along[n], 0, me).wait_recv()
            for m in range(3):
                key_copy(along[n], 12 + 3 * n + m, across[m]).start()
            value_copy(across[n], 0, me).wait_recv()
            for m in range(3):
                value_copy(across[n], 21 + 3 * n + m, along[m]).start()

    for n in range(3):
        for m in range(3):
            passed.append(key_copy(along[n], 12 + 3 * n + m, across[m]))
            passed.append(value_copy(across[n], 21 + 3 * n + m, along[m]))

    def arrived(block):
        @pl.when(block // 4 != row)
        def _():
            key_copy(block, 0, me).wait_recv()

        @pl.when(block % 4 != column)
        def _():
            value_copy(block, 0, me).wait_recv()

    def unit(which, place, diagonal):
        block, side = place // 2, place % 2
        for part in (1, 0):
            at = (2 * side + part) * 128
            left = key_ref[block, pl.ds(at, HEAD_DIM), :]
            right = key_ref[block, pl.ds(at + HEAD_DIM, HEAD_DIM), :]
            keys = jnp.concatenate([left, right], axis=1)
            keys = jnp.concatenate([keys, keys], axis=0)
            values = value_ref[block, pl.ds(part * TILE, TILE), :]
            lanes = lax.broadcasted_iota(jnp.int32, values.shape, 1) // HEAD_DIM
            values = jnp.where(lanes == side, values, jnp.zeros_like(values))
            rows, mask = pl.ds(0, half), None
            if diagonal and part == 1:
                rows, mask = pl.ds(TILE, TILE), c < r
            elif diagonal:
                mask = lax.broadcasted_iota(jnp.int32, (half, TILE), 1) < lax.broadcasted_iota(
                    jnp.int32, (half, TILE), 0
                )
            out, carry = tile_terms(
                q_ref2[which, rows, :], keys, values, tri_ref[...], carry_ref[which, block, rows, :], mask
            )
            acc_ref[which, block, rows, :] += out
            carry_ref[which, block, rows, :] = carry

    def finish(which, place):
        blank = jnp.zeros((half, 128), jnp.float32)
        sum_ref[...] = blank
        past_ref[...] = blank

        def later(n, unused):
            block = place // 2 - n
            sum_ref[...] += jnp.exp2(-past_ref[...]) * acc_ref[which, block]
            past_ref[...] += carry_ref[which, block]
            return unused

        lax.fori_loop(0, place // 2 + 1, later, 0)
        acc = sum_ref[...]
        mixed = acc[:, :HEAD_DIM] + acc[:, HEAD_DIM:]
        inverse = lax.rsqrt(jnp.mean(mixed * mixed, axis=1, keepdims=True) + EPSILON)
        normed = mixed * inverse * gain_ref[...]
        for piece in range(4):
            at = piece * 128
            two = jnp.concatenate([normed[at : at + 64], normed[at + 64 : at + 128]], axis=1)
            out_own[4 * which + piece] = two.astype(jnp.bfloat16)
        for piece in range(4):
            n = 4 * which + piece
            where, token = place // 2, (place % 2) * 4 + piece
            mine = (where == me) & (token == head)

            @pl.when(jnp.logical_not(mine))
            def _():
                copy(out_own.at[n], out_in.at[head], out_send.at[n], out_recv.at[head], where, token).start()

            @pl.when(mine)
            def _():
                pltpu.make_async_copy(out_own.at[n], out_in.at[head], out_local).start()

    far = jnp.maximum(2 * me, 31 - 2 * me)
    order = ((0, 0), (0, 1), (1, 0), (0, 3), (3, 0), (0, 2), (2, 0), (1, 1), (3, 3), (1, 3), (3, 1), (1, 2), (2, 1), (3, 2), (2, 3), (2, 2))

    def pick(n, axis):
        return sum(jnp.where(n == k, one[axis], 0) for k, one in enumerate(order))

    def visit(n, unused):
        block = (row + pick(n, 0)) % 4 * 4 + (column + pick(n, 1)) % 4

        @pl.when(n == 1)
        def _():
            forward()

        @pl.when(n == 10)
        def _():
            spread(outgoing, arrived_ref, row_send, row_recv, row_local, me * 8 + head)

        @pl.when((block <= far // 2) & (n > 0))
        def _():
            arrived(block)

        def pair(i, unused):
            which, side = i // 2, 1 - i % 2
            top = jnp.where(which == 0, 2 * me, 31 - 2 * me)
            place = 2 * block + side

            @pl.when((n == 0) & (i == 2))
            def _():
                q_copy.wait_recv()

            @pl.when((side == 1) & (2 * block <= top))
            def _():
                acc_ref[which, block] = jnp.zeros((half, 128), jnp.float32)
                carry_ref[which, block] = jnp.zeros((half, 128), jnp.float32)

            @pl.when(place < top)
            def _():
                unit(which, place, False)

            @pl.when(place == top)
            def _():
                unit(which, place, True)

            return unused

        @pl.when(block <= far // 2)
        def _():
            lax.fori_loop(0, 4, pair, 0)

        return unused

    lax.fori_loop(0, 16, visit, 0)
    finish(0, 2 * me)
    finish(1, 31 - 2 * me)

    def drain(n, unused):
        @pl.when(n != me)
        def _():
            arrived(n)

        return unused

    lax.fori_loop(far // 2 + 1, 16, drain, 0)
    q_copy.wait_send()
    for one in sent + passed:
        one.wait_send()

    for other in range(8):
        @pl.when(jnp.logical_not((head < 4) & (other == head)))
        def _():
            copy(out_own.at[0], out_in.at[other], out_send.at[0], out_recv.at[other], me, head).wait_recv()
    for which, spot in ((0, 2 * me), (1, 31 - 2 * me)):
        for piece in range(4):
            n = 4 * which + piece
            where, token = spot // 2, (spot % 2) * 4 + piece
            mine = (where == me) & (token == head)

            @pl.when(jnp.logical_not(mine))
            def _():
                copy(out_own.at[n], out_in.at[head], out_send.at[n], out_recv.at[head], where, token).wait_send()

            @pl.when(mine)
            def _():
                pltpu.make_async_copy(out_own.at[n], out_in.at[head], out_local).wait()

    for pair in range(4):
        one = out_in[2 * pair].astype(jnp.float32)
        two = out_in[2 * pair + 1].astype(jnp.float32)
        one = jnp.concatenate([one[:, :HEAD_DIM], one[:, HEAD_DIM:]], axis=0)
        two = jnp.concatenate([two[:, :HEAD_DIM], two[:, HEAD_DIM:]], axis=0)
        out_ref[:, pl.ds(pair * 128, 128)] = jnp.concatenate([one, two], axis=1).astype(jnp.bfloat16)
    spread_own(outgoing, arrived_ref, row_local, me * 8 + head)
    spread_wait(arrived_ref, row_recv)
    spread_wait(outgoing, row_send)


def attention(queries, key_heads, value_heads, head_gain, residual, routed_experts):
    rows = queries.shape[0]
    half = rows // 2
    return pl.pallas_call(
        attention_kernel,
        out_shape=(
            jax.ShapeDtypeStruct((128, 8 * HEAD_DIM), jnp.bfloat16),
            jax.ShapeDtypeStruct((128, 48, 128), jnp.bfloat16),
        ),
        in_specs=[pl.BlockSpec(memory_space=pltpu.VMEM)] * 6,
        out_specs=[pl.BlockSpec(memory_space=pltpu.VMEM)] * 2,
        scratch_shapes=[
            pltpu.VMEM((half, 128), jnp.bfloat16),
            pltpu.VMEM((2, half, 128), jnp.bfloat16),
            pltpu.VMEM((16, half, 128), jnp.bfloat16),
            pltpu.VMEM((16, half, 128), jnp.bfloat16),
            pltpu.VMEM((2, 16, half, 128), jnp.float32),
            pltpu.VMEM((2, 16, half, 128), jnp.float32),
            pltpu.VMEM((half, 128), jnp.float32),
            pltpu.VMEM((half, 128), jnp.float32),
            pltpu.VMEM((TILE, TILE), jnp.bfloat16),
            pltpu.VMEM((8, 64, 128), jnp.bfloat16),
            pltpu.VMEM((8, 64, 128), jnp.bfloat16),
            pltpu.VMEM((2, 3, 128, 128), jnp.bfloat16),
            pltpu.VMEM((128 * 48, 128), jnp.float32),
            pltpu.VMEM((128, 48, 128), jnp.bfloat16),
            pltpu.SemaphoreType.DMA,
            pltpu.SemaphoreType.DMA,
            pltpu.SemaphoreType.DMA((30,)),
            pltpu.SemaphoreType.DMA((16,)),
            pltpu.SemaphoreType.DMA((16,)),
            pltpu.SemaphoreType.DMA((8,)),
            pltpu.SemaphoreType.DMA((8,)),
            pltpu.SemaphoreType.DMA,
            pltpu.SemaphoreType.DMA,
            pltpu.SemaphoreType.DMA,
            pltpu.SemaphoreType.DMA,
        ],
        compiler_params=pltpu.CompilerParams(vmem_limit_bytes=56 << 20, has_side_effects=True),
        name="attention",
    )(queries.T, key_heads.T, value_heads.T, head_gain.reshape(1, HEAD_DIM), residual, routed_experts)


def mixture_kernel(
    head_ref, arrived, residual_ref, gain_ref, expert_ref, route_ref,
    out_weight, shared_gate, shared_up, shared_down, expert_gate, expert_up, expert_down,
    final_ref,
    ow_ref, sg_ref, su_ref, sd_ref, eg_ref, eu_ref, ed_ref,
    stream_ref, x_ref, place_ref, mix_ref, stage_ref, head_stage, head_out, head_in, head_rows,
    rows_ref, hidden_ref, outgoing, incoming,
    result, returned, total_ref,
    load_sem, head_send, head_recv, head_local, row_send, row_recv, row_local, back_send, back_recv, local_sem,
):
    me = lax.axis_index("sp") * 8 + lax.axis_index("tp")
    tokens, width = residual_ref.shape
    devices, slots = 128, 3
    chunks = width // 128
    hidden = sg_ref.shape[1]
    f32, bf16 = jnp.float32, jnp.bfloat16

    loads = [
        pltpu.make_async_copy(source, target, load_sem.at[n])
        for n, (source, target) in enumerate(
            (
                (out_weight, ow_ref), (shared_gate, sg_ref), (shared_up, su_ref), (shared_down, sd_ref),
                (expert_gate, eg_ref), (expert_up, eu_ref), (expert_down, ed_ref),
            )
        )
    ]
    for one in loads:
        one.start()

    route(expert_ref, route_ref, place_ref, mix_ref)
    head_stage[...] = jnp.zeros_like(head_stage)
    for slot in range(slots):
        rows = jnp.dot(place_ref[0, slot], head_ref[...], preferred_element_type=f32)
        for k in range(4):
            head_stage[pl.ds(slot * 4 + k, devices, stride=16), :] = rows[:, k * 128 : (k + 1) * 128]

    def pack(n, unused):
        block = head_stage[pl.ds(n * 128, 128), :].astype(bf16)
        for k in range(8):
            head_out[n * 8 + k] = block[k * 16 : (k + 1) * 16]
        return unused

    lax.fori_loop(0, devices // 8, pack, 0)
    spread(head_out, head_in, head_send, head_recv, head_local, me)

    loads[0].wait()
    squares = jnp.zeros((tokens, 1), f32)
    for n in range(width // 512):
        at = pl.ds(n * 512, 512)
        branch = jnp.dot(head_ref[...], ow_ref[:, at], preferred_element_type=f32)
        stream = (residual_ref[:, at].astype(f32) + branch).astype(bf16).astype(f32)
        stream_ref[:, at] = stream
        squares = squares + jnp.sum(stream * stream, axis=1, keepdims=True)
    inverse = lax.rsqrt(squares / width + EPSILON)
    for n in range(width // 512):
        at = pl.ds(n * 512, 512)
        x_ref[:, at] = (stream_ref[:, at] * inverse * gain_ref[:, at]).astype(bf16)

    collect(place_ref, 1, x_ref, stage_ref, outgoing)
    spread(outgoing, incoming, row_send, row_recv, row_local, me)

    def stage_to(target, side):
        def one(n, unused):
            block = stage_ref[pl.ds(n * 384, 384), :].astype(bf16)
            for k in range(8):
                target[side, n * 8 + k] = block[k * 48 : (k + 1) * 48]
            return unused

        lax.fori_loop(0, devices // 8, one, 0)

    def stage_from(source):
        def one(n, unused):
            for k in range(8):
                at = n * 384 + k * 48
                stage_ref[pl.ds(at, 48), :] = source(n * 8 + k).astype(f32)
            return unused

        lax.fori_loop(0, devices // 8, one, 0)

    def exchange(source, target, send, receive, side):
        spread(source.at[side], target.at[side], send.at[side], receive.at[side], local_sem, me)
        spread_own(source.at[side], target.at[side], local_sem, me)

    def wait_all(buffer, sem, side):
        everyone = buffer.at[side, pl.ds(0, devices - 1)]
        pltpu.make_async_copy(everyone, everyone, sem.at[side]).wait()

    for one in loads[1:4]:
        one.wait()
    gate = jnp.dot(x_ref[...], sg_ref[...], preferred_element_type=f32)
    up = jnp.dot(x_ref[...], su_ref[...], preferred_element_type=f32)
    shared = (gate / (1.0 + jnp.exp(-gate)) * up).astype(bf16)
    for n in range(width // 512):
        at = pl.ds(n * 512, 512)
        total_ref[:, at] = stream_ref[:, at] + jnp.dot(
            shared, sd_ref[:, at], preferred_element_type=f32
        )
    for one in loads[4:]:
        one.wait()

    spread_own(head_out, head_in, head_local, me)
    spread_wait(head_in, head_recv)

    def unpack(n, unused):
        for k in range(8):
            head_stage[pl.ds(n * 128 + k * 16, 16), :] = head_in[n * 8 + k].astype(f32)
        return unused

    lax.fori_loop(0, devices // 8, unpack, 0)

    def first_rows():
        stage_from(lambda at: arrived[at])
        for slot in range(slots):
            for k in range(4):
                head_rows[pl.ds(slot * devices, devices), pl.ds(k * 128, 128)] = head_stage[
                    pl.ds(slot * 4 + k, devices, stride=16), :
                ].astype(bf16)
        for slot in range(slots):
            rows = pl.ds(slot * devices, devices)
            squares = jnp.zeros((devices, 1), f32)
            for n in range(width // 512):
                at = pl.ds(n * 512, 512)
                branch = jnp.dot(head_rows[rows, :], ow_ref[:, at], preferred_element_type=f32)
                base = jnp.concatenate(
                    [
                        stage_ref[pl.ds(slot * chunks + n * 4 + k, devices, stride=slots * chunks), :]
                        for k in range(4)
                    ],
                    axis=1,
                )
                stream = (base + branch).astype(bf16)
                rows_ref[rows, at] = stream
                stream = stream.astype(f32)
                squares = squares + jnp.sum(stream * stream, axis=1, keepdims=True)
            inverse = lax.rsqrt(squares / width + EPSILON)
            for n in range(width // 512):
                at = pl.ds(n * 512, 512)
                rows_ref[rows, at] = (rows_ref[rows, at].astype(f32) * inverse * gain_ref[:, at]).astype(bf16)

    def second_rows():
        spread_own(outgoing, incoming, row_local, me)
        spread_wait(incoming, row_recv)
        stage_from(lambda at: incoming[at])
        for slot in range(slots):
            for k in range(chunks):
                rows_ref[pl.ds(slot * devices, devices), pl.ds(k * 128, 128)] = stage_ref[
                    pl.ds(slot * chunks + k, devices, stride=slots * chunks), :
                ].astype(bf16)

    for side in range(2):
        (first_rows, second_rows)[side]()

        def inner(n, unused):
            at = pl.ds(pl.multiple_of(n * 256, 256), 256)
            gate = jnp.dot(rows_ref[...], eg_ref[side, :, at], preferred_element_type=f32)
            up = jnp.dot(rows_ref[...], eu_ref[side, :, at], preferred_element_type=f32)
            hidden_ref[:, at] = (gate / (1.0 + jnp.exp(-gate)) * up).astype(bf16)
            return unused

        lax.fori_loop(0, hidden // 256, inner, 0)

        def outer(n, unused):
            at = pl.ds(pl.multiple_of(n * 256, 256), 256)
            rows = jnp.dot(hidden_ref[...], ed_ref[side, :, at], preferred_element_type=f32)
            for slot in range(slots):
                for k in range(2):
                    stage_ref[pl.ds(slot * chunks + n * 2 + k, devices, stride=slots * chunks), :] = (
                        rows[slot * devices : (slot + 1) * devices, k * 128 : (k + 1) * 128]
                    )
            return unused

        lax.fori_loop(0, width // 256, outer, 0)
        stage_to(result, side)
        exchange(result, returned, back_send, back_recv, side)

    for side in range(2):
        wait_all(returned, back_recv, side)
        stage_from(lambda at: returned[side, at])
        for k in range(chunks):
            at = pl.ds(k * 128, 128)
            total = total_ref[:, at]
            for slot in range(slots):
                rows = stage_ref[pl.ds(slot * chunks + k, devices, stride=slots * chunks), :].astype(bf16)
                for level in range(2):
                    total = total + jnp.dot(
                        mix_ref[level, side, slot], rows, preferred_element_type=f32
                    )
            total_ref[:, at] = total
    final_ref[...] = total_ref[...].astype(bf16)
    spread_wait(head_out, head_send)
    spread_wait(outgoing, row_send)
    for side in range(2):
        wait_all(result, back_send, side)


def mixture(
    heads, arrived, residual, out_weight, norm_gain, shared_gate, shared_up, shared_down,
    expert_gate, expert_up, expert_down, routed_experts, route_weights,
):
    tokens, width = residual.shape
    hidden = shared_gate.shape[1]
    bf16, f32 = jnp.bfloat16, jnp.float32
    vmem, anywhere = pl.BlockSpec(memory_space=pltpu.VMEM), pl.BlockSpec(memory_space=pl.ANY)
    blocks = (2, 128, 48, 128)
    return pl.pallas_call(
        mixture_kernel,
        out_shape=jax.ShapeDtypeStruct((tokens, width), bf16),
        in_specs=[vmem] * 6 + [anywhere] * 7,
        out_specs=vmem,
        scratch_shapes=[
            pltpu.VMEM(out_weight.shape, bf16),
            pltpu.VMEM(shared_gate.shape, bf16),
            pltpu.VMEM(shared_up.shape, bf16),
            pltpu.VMEM(shared_down.shape, bf16),
            pltpu.VMEM(expert_gate.shape, bf16),
            pltpu.VMEM(expert_up.shape, bf16),
            pltpu.VMEM(expert_down.shape, bf16),
            pltpu.VMEM((tokens, width), f32),
            pltpu.VMEM((tokens, width), bf16),
            pltpu.VMEM((2, 3, 128, tokens), bf16),
            pltpu.VMEM((2, 2, 3, tokens, 128), bf16),
            pltpu.VMEM((128 * 48, 128), f32),
            pltpu.VMEM((128 * 16, 128), f32),
            pltpu.VMEM((128, 16, 128), bf16),
            pltpu.VMEM((128, 16, 128), bf16),
            pltpu.VMEM((384, 512), bf16),
            pltpu.VMEM((384, width), bf16),
            pltpu.VMEM((384, hidden), bf16),
            pltpu.VMEM((128, 48, 128), bf16),
            pltpu.VMEM((128, 48, 128), bf16),
            pltpu.VMEM(blocks, bf16),
            pltpu.VMEM(blocks, bf16),
            pltpu.VMEM((tokens, width), f32),
            pltpu.SemaphoreType.DMA((7,)),
            pltpu.SemaphoreType.DMA,
            pltpu.SemaphoreType.DMA,
            pltpu.SemaphoreType.DMA,
            pltpu.SemaphoreType.DMA,
            pltpu.SemaphoreType.DMA,
            pltpu.SemaphoreType.DMA,
            pltpu.SemaphoreType.DMA((2,)),
            pltpu.SemaphoreType.DMA((2,)),
            pltpu.SemaphoreType.DMA,
        ],
        compiler_params=pltpu.CompilerParams(vmem_limit_bytes=60 << 20, has_side_effects=True),
        name="mixture",
    )(
        heads, arrived, residual, norm_gain.reshape(1, width), routed_experts, route_weights.T,
        out_weight, shared_gate, shared_up, shared_down, expert_gate, expert_up, expert_down,
    )


def body(
    queries,
    key_heads,
    value_heads,
    head_gain,
    residual,
    out_weight,
    norm_gain,
    shared_gate,
    shared_up,
    shared_down,
    expert_gate,
    expert_up,
    expert_down,
    routed_experts,
    route_weights,
):
    experts = routed_experts.T
    heads, arrived = attention(queries, key_heads, value_heads, head_gain, residual, experts)
    return mixture(
        heads,
        arrived,
        residual,
        out_weight,
        norm_gain,
        shared_gate,
        shared_up,
        shared_down,
        expert_gate,
        expert_up,
        expert_down,
        experts,
        route_weights,
    )


def solution(mesh):
    return jax.shard_map(
        body,
        mesh=mesh,
        in_specs=(
            P("sp", "tp"),
            P("sp", "tp"),
            P("sp", "tp"),
            P("tp"),
            P(("sp", "tp"), None),
            P(),
            P(),
            P(),
            P(),
            P(),
            P(("sp", "tp"), None, None),
            P(("sp", "tp"), None, None),
            P(("sp", "tp"), None, None),
            P(("sp", "tp"), None),
            P(("sp", "tp"), None),
        ),
        out_specs=P(("sp", "tp"), None),
        check_vma=False,
    )
```

```python
import math

import jax
import jax.numpy as jnp
from jax import lax
from jax.experimental import pallas as pl
from jax.experimental.pallas import tpu as pltpu
from jax.sharding import PartitionSpec as P

HEAD_DIM = 64


EPSILON = 1e-06


LOG2E = 1.4426950408889634
TILE = 256
MESH = pl.DeviceIdType.MESH


def tile_terms(q2, keys, values, tri, carry, mask):
    x = jnp.dot(q2, keys, preferred_element_type=jnp.float32)
    x = jnp.minimum(x, 126.0)
    drop = jnp.log(1.0 + jnp.exp2(x)) * LOG2E
    stick = x - drop
    if mask is not None:
        drop = jnp.where(mask, drop, 0.0)
    after = jnp.dot(drop.astype(jnp.bfloat16), tri, preferred_element_type=jnp.float32)
    both = jnp.concatenate([carry, carry], axis=1)
    weights = jnp.exp2(stick - after - both)
    if mask is not None:
        weights = jnp.where(mask, weights, 0.0)
    out = jnp.dot(weights.astype(jnp.bfloat16), values, preferred_element_type=jnp.float32)
    total = after[:, :1] + drop[:, :1]
    return out, carry + jnp.broadcast_to(total, carry.shape)


def remote(source, target, send, receive, where):
    return pltpu.make_async_remote_copy(
        src_ref=source, dst_ref=target, send_sem=send, recv_sem=receive,
        device_id=where, device_id_type=MESH,
    )


def route(expert_ref, route_ref, place_ref, mix_ref):
    devices, slots, tokens = 128, 3, expert_ref.shape[1]
    f32, bf16 = jnp.float32, jnp.bfloat16
    line = lax.broadcasted_iota(jnp.int32, (2 * devices, tokens), 0)
    expert = 2 * (line % devices) + line // devices
    named = jnp.zeros((2 * devices, tokens), f32)
    weight = jnp.zeros((2 * devices, tokens), f32)
    for pick in range(expert_ref.shape[0]):
        hit = expert_ref[pick : pick + 1, :] == expert
        named = named + jnp.where(hit, 1.0, 0.0)
        if mix_ref is not None:
            weight = weight + jnp.where(hit, route_ref[pick : pick + 1, :], 0.0)
    before = lax.broadcasted_iota(jnp.int32, (tokens, tokens), 0) < lax.broadcasted_iota(
        jnp.int32, (tokens, tokens), 1
    )
    rank = jnp.dot(
        named.astype(bf16), jnp.where(before, 1.0, 0.0).astype(bf16), preferred_element_type=f32
    )
    for slot in range(slots):
        chosen = jnp.where(rank == float(slot), named, 0.0)
        for side in range(2):
            part = chosen[side * devices : (side + 1) * devices]
            place_ref[side, slot] = part.astype(bf16)
            if mix_ref is not None:
                mix = (part * weight[side * devices : (side + 1) * devices]).T
                high = mix.astype(bf16)
                mix_ref[0, side, slot] = high
                mix_ref[1, side, slot] = (mix - high.astype(f32)).astype(bf16)


def collect(place_ref, side, from_ref, stage_ref, outgoing):
    for slot in range(3):
        place = place_ref[side, slot]

        def gather(n, unused):
            at = pl.multiple_of(n * 512, 512)
            rows = jnp.dot(place, from_ref[:, pl.ds(at, 512)], preferred_element_type=jnp.float32)
            for k in range(4):
                stage_ref[pl.ds(slot * 16 + n * 4 + k, 128, stride=48), :] = (
                    rows[:, k * 128 : (k + 1) * 128]
                )
            return unused

        lax.fori_loop(0, from_ref.shape[1] // 512, gather, 0)

    def move(n, unused):
        block = stage_ref[pl.ds(n * 384, 384), :].astype(jnp.bfloat16)
        for k in range(8):
            outgoing[n * 8 + k] = block[k * 48 : (k + 1) * 48]
        return unused

    lax.fori_loop(0, 16, move, 0)


def spread(source, target, send, receive, own, me):
    def go(n):
        where = lax.rem(me + 37 * n, 128)
        device = (lax.div(where, 8), lax.rem(where, 8))
        remote(source.at[where], target.at[me], send, receive, device).start()

    def several(n, unused):
        for k in range(7):
            go(7 * n + k + 1)
        return unused

    lax.fori_loop(0, 18, several, 0)
    go(127)
    pltpu.make_async_copy(source.at[me], target.at[me], own).start()


def spread_own(source, target, own, me):
    pltpu.make_async_copy(source.at[me], target.at[me], own).wait()


def spread_wait(buffer, sem):
    everyone = buffer.at[pl.ds(0, 127)]
    pltpu.make_async_copy(everyone, everyone, sem).wait()


def attention_kernel(
    q_ref, k_ref, v_ref, gain_ref, residual_ref, expert_ref, out_ref, arrived_ref,
    q_own, q_ref2, key_ref, value_ref, acc_ref, carry_ref, sum_ref, past_ref, tri_ref, out_own, out_in,
    place_ref, stage_ref, outgoing,
    q_send, q_recv, send_sem, key_recv, value_recv, out_send, out_recv, out_local,
    row_send, row_recv, row_local,
):
    me, head = lax.axis_index("sp"), lax.axis_index("tp")
    row, column = me // 4, me % 4
    half = q_ref.shape[1] // 2

    q = q_ref[...].astype(jnp.float32).T * (LOG2E / math.sqrt(HEAD_DIM))
    high = q.astype(jnp.bfloat16)
    low = (q - high.astype(jnp.float32)).astype(jnp.bfloat16)
    both = jnp.concatenate([high, low], axis=1)
    q_ref2[0] = both[:half]
    q_own[...] = both[half:]
    for part in range(8):
        key_ref[me, pl.ds(part * HEAD_DIM, HEAD_DIM), :] = k_ref[:, pl.ds(part * 128, 128)]
    v = v_ref[...].astype(jnp.float32).T
    value_ref[me] = jnp.concatenate([v[:half], v[half:]], axis=1).astype(jnp.bfloat16)

    def copy(source, target, out_sem, in_sem, where, which):
        return pltpu.make_async_remote_copy(
            src_ref=source, dst_ref=target, send_sem=out_sem, recv_sem=in_sem,
            device_id=(where, which), device_id_type=MESH,
        )

    q_copy = copy(q_own, q_ref2.at[1], q_send, q_recv, 15 - me, head)
    q_copy.start()
    steps = (1, 3, 2)

    def key_copy(block, n, where):
        return copy(key_ref.at[block], key_ref.at[block], send_sem.at[n], key_recv.at[block], where, head)

    def value_copy(block, n, where):
        return copy(value_ref.at[block], value_ref.at[block], send_sem.at[n], value_recv.at[block], where, head)

    along = [row * 4 + (column + d) % 4 for d in steps]
    across = [(row + d) % 4 * 4 + column for d in steps]
    sent = []
    for n in range(3):
        sent.append(key_copy(me, n, along[n]))
        sent.append(value_copy(me, 3 + n, across[n]))
    for n in range(3):
        sent.append(key_copy(me, 6 + n, across[n]))
        sent.append(value_copy(me, 9 + n, along[n]))
    for one in sent:
        one.start()

    r = lax.broadcasted_iota(jnp.int32, (TILE, TILE), 0)
    c = lax.broadcasted_iota(jnp.int32, (TILE, TILE), 1)
    tri_ref[...] = (r > c).astype(jnp.float32).astype(jnp.bfloat16)
    route(expert_ref, None, place_ref, None)
    collect(place_ref, 0, residual_ref, stage_ref, outgoing)

    passed = []

    def forward():
        for n in range(3):
            key_copy(along[n], 0, me).wait_recv()
            for m in range(3):
                key_copy(along[n], 12 + 3 * n + m, across[m]).start()
            value_copy(across[n], 0, me).wait_recv()
            for m in range(3):
                value_copy(across[n], 21 + 3 * n + m, along[m]).start()

    for n in range(3):
        for m in range(3):
            passed.append(key_copy(along[n], 12 + 3 * n + m, across[m]))
            passed.append(value_copy(across[n], 21 + 3 * n + m, along[m]))

    def arrived(block):
        @pl.when(block // 4 != row)
        def _():
            key_copy(block, 0, me).wait_recv()

        @pl.when(block % 4 != column)
        def _():
            value_copy(block, 0, me).wait_recv()

    def unit(which, place, diagonal):
        block, side = place // 2, place % 2
        for part in (1, 0):
            at = (2 * side + part) * 128
            left = key_ref[block, pl.ds(at, HEAD_DIM), :]
            right = key_ref[block, pl.ds(at + HEAD_DIM, HEAD_DIM), :]
            keys = jnp.concatenate([left, right], axis=1)
            keys = jnp.concatenate([keys, keys], axis=0)
            values = value_ref[block, pl.ds(part * TILE, TILE), :]
            lanes = lax.broadcasted_iota(jnp.int32, values.shape, 1) // HEAD_DIM
            values = jnp.where(lanes == side, values, jnp.zeros_like(values))
            rows, mask = pl.ds(0, half), None
            if diagonal and part == 1:
                rows, mask = pl.ds(TILE, TILE), c < r
            elif diagonal:
                mask = lax.broadcasted_iota(jnp.int32, (half, TILE), 1) < lax.broadcasted_iota(
                    jnp.int32, (half, TILE), 0
                )
            out, carry = tile_terms(
                q_ref2[which, rows, :], keys, values, tri_ref[...], carry_ref[which, block, rows, :], mask
            )
            acc_ref[which, block, rows, :] += out
            carry_ref[which, block, rows, :] = carry

    def finish(which, place):
        blank = jnp.zeros((half, 128), jnp.float32)
        sum_ref[...] = blank
        past_ref[...] = blank

        def later(n, unused):
            block = place // 2 - n
            sum_ref[...] += jnp.exp2(-past_ref[...]) * acc_ref[which, block]
            past_ref[...] += carry_ref[which, block]
            return unused

        lax.fori_loop(0, place // 2 + 1, later, 0)
        acc = sum_ref[...]
        mixed = acc[:, :HEAD_DIM] + acc[:, HEAD_DIM:]
        inverse = lax.rsqrt(jnp.mean(mixed * mixed, axis=1, keepdims=True) + EPSILON)
        normed = mixed * inverse * gain_ref[...]
        for piece in range(4):
            at = piece * 128
            two = jnp.concatenate([normed[at : at + 64], normed[at + 64 : at + 128]], axis=1)
            out_own[4 * which + piece] = two.astype(jnp.bfloat16)
        for piece in range(4):
            n = 4 * which + piece
            where, token = place // 2, (place % 2) * 4 + piece
            mine = (where == me) & (token == head)

            @pl.when(jnp.logical_not(mine))
            def _():
                copy(out_own.at[n], out_in.at[head], out_send.at[n], out_recv.at[head], where, token).start()

            @pl.when(mine)
            def _():
                pltpu.make_async_copy(out_own.at[n], out_in.at[head], out_local).start()

    far = jnp.maximum(2 * me, 31 - 2 * me)
    order = ((0, 0), (0, 1), (1, 0), (0, 3), (3, 0), (0, 2), (2, 0), (1, 1), (3, 3), (1, 3), (3, 1), (1, 2), (2, 1), (3, 2), (2, 3), (2, 2))

    def pick(n, axis):
        return sum(jnp.where(n == k, one[axis], 0) for k, one in enumerate(order))

    def visit(n, unused):
        block = (row + pick(n, 0)) % 4 * 4 + (column + pick(n, 1)) % 4

        @pl.when(n == 1)
        def _():
            forward()

        @pl.when(n == 10)
        def _():
            spread(outgoing, arrived_ref, row_send, row_recv, row_local, me * 8 + head)

        @pl.when((block <= far // 2) & (n > 0))
        def _():
            arrived(block)

        def pair(i, unused):
            which, side = i // 2, 1 - i % 2
            top = jnp.where(which == 0, 2 * me, 31 - 2 * me)
            place = 2 * block + side

            @pl.when((n == 0) & (i == 2))
            def _():
                q_copy.wait_recv()

            @pl.when((side == 1) & (2 * block <= top))
            def _():
                acc_ref[which, block] = jnp.zeros((half, 128), jnp.float32)
                carry_ref[which, block] = jnp.zeros((half, 128), jnp.float32)

            @pl.when(place < top)
            def _():
                unit(which, place, False)

            @pl.when(place == top)
            def _():
                unit(which, place, True)

            return unused

        @pl.when(block <= far // 2)
        def _():
            lax.fori_loop(0, 4, pair, 0)

        return unused

    lax.fori_loop(0, 16, visit, 0)
    finish(0, 2 * me)
    finish(1, 31 - 2 * me)

    def drain(n, unused):
        @pl.when(n != me)
        def _():
            arrived(n)

        return unused

    lax.fori_loop(far // 2 + 1, 16, drain, 0)
    q_copy.wait_send()
    for one in sent + passed:
        one.wait_send()

    for other in range(8):
        @pl.when(jnp.logical_not((head < 4) & (other == head)))
        def _():
            copy(out_own.at[0], out_in.at[other], out_send.at[0], out_recv.at[other], me, head).wait_recv()
    for which, spot in ((0, 2 * me), (1, 31 - 2 * me)):
        for piece in range(4):
            n = 4 * which + piece
            where, token = spot // 2, (spot % 2) * 4 + piece
            mine = (where == me) & (token == head)

            @pl.when(jnp.logical_not(mine))
            def _():
                copy(out_own.at[n], out_in.at[head], out_send.at[n], out_recv.at[head], where, token).wait_send()

            @pl.when(mine)
            def _():
                pltpu.make_async_copy(out_own.at[n], out_in.at[head], out_local).wait()

    for pair in range(4):
        one = out_in[2 * pair].astype(jnp.float32)
        two = out_in[2 * pair + 1].astype(jnp.float32)
        one = jnp.concatenate([one[:, :HEAD_DIM], one[:, HEAD_DIM:]], axis=0)
        two = jnp.concatenate([two[:, :HEAD_DIM], two[:, HEAD_DIM:]], axis=0)
        out_ref[:, pl.ds(pair * 128, 128)] = jnp.concatenate([one, two], axis=1).astype(jnp.bfloat16)
    spread_own(outgoing, arrived_ref, row_local, me * 8 + head)
    spread_wait(arrived_ref, row_recv)
    spread_wait(outgoing, row_send)


def attention(queries, key_heads, value_heads, head_gain, residual, routed_experts):
    rows = queries.shape[0]
    half = rows // 2
    return pl.pallas_call(
        attention_kernel,
        out_shape=(
            jax.ShapeDtypeStruct((128, 8 * HEAD_DIM), jnp.bfloat16),
            jax.ShapeDtypeStruct((128, 48, 128), jnp.bfloat16),
        ),
        in_specs=[pl.BlockSpec(memory_space=pltpu.VMEM)] * 6,
        out_specs=[pl.BlockSpec(memory_space=pltpu.VMEM)] * 2,
        scratch_shapes=[
            pltpu.VMEM((half, 128), jnp.bfloat16),
            pltpu.VMEM((2, half, 128), jnp.bfloat16),
            pltpu.VMEM((16, half, 128), jnp.bfloat16),
            pltpu.VMEM((16, half, 128), jnp.bfloat16),
            pltpu.VMEM((2, 16, half, 128), jnp.float32),
            pltpu.VMEM((2, 16, half, 128), jnp.float32),
            pltpu.VMEM((half, 128), jnp.float32),
            pltpu.VMEM((half, 128), jnp.float32),
            pltpu.VMEM((TILE, TILE), jnp.bfloat16),
            pltpu.VMEM((8, 64, 128), jnp.bfloat16),
            pltpu.VMEM((8, 64, 128), jnp.bfloat16),
            pltpu.VMEM((2, 3, 128, 128), jnp.bfloat16),
            pltpu.VMEM((128 * 48, 128), jnp.float32),
            pltpu.VMEM((128, 48, 128), jnp.bfloat16),
            pltpu.SemaphoreType.DMA,
            pltpu.SemaphoreType.DMA,
            pltpu.SemaphoreType.DMA((30,)),
            pltpu.SemaphoreType.DMA((16,)),
            pltpu.SemaphoreType.DMA((16,)),
            pltpu.SemaphoreType.DMA((8,)),
            pltpu.SemaphoreType.DMA((8,)),
            pltpu.SemaphoreType.DMA,
            pltpu.SemaphoreType.DMA,
            pltpu.SemaphoreType.DMA,
            pltpu.SemaphoreType.DMA,
        ],
        compiler_params=pltpu.CompilerParams(vmem_limit_bytes=56 << 20, has_side_effects=True),
        name="attention",
    )(queries.T, key_heads.T, value_heads.T, head_gain.reshape(1, HEAD_DIM), residual, routed_experts)


def mixture_kernel(
    head_ref, arrived, residual_ref, gain_ref, expert_ref, route_ref,
    out_weight, shared_gate, shared_up, shared_down, expert_gate, expert_up, expert_down,
    final_ref,
    ow_ref, sg_ref, su_ref, sd_ref, eg_ref, eu_ref, ed_ref,
    stream_ref, x_ref, place_ref, mix_ref, stage_ref, head_stage, head_out, head_in, head_rows,
    rows_ref, hidden_ref, outgoing, incoming,
    result, returned, total_ref,
    load_sem, head_send, head_recv, head_local, row_send, row_recv, row_local, back_send, back_recv, local_sem,
):
    me = lax.axis_index("sp") * 8 + lax.axis_index("tp")
    tokens, width = residual_ref.shape
    devices, slots = 128, 3
    chunks = width // 128
    hidden = sg_ref.shape[1]
    f32, bf16 = jnp.float32, jnp.bfloat16

    loads = [
        pltpu.make_async_copy(source, target, load_sem.at[n])
        for n, (source, target) in enumerate(
            (
                (out_weight, ow_ref), (shared_gate, sg_ref), (shared_up, su_ref), (shared_down, sd_ref),
                (expert_gate, eg_ref), (expert_up, eu_ref), (expert_down, ed_ref),
            )
        )
    ]
    for one in loads:
        one.start()

    route(expert_ref, None, place_ref, None)
    head_stage[...] = jnp.zeros_like(head_stage)
    for slot in range(slots):
        rows = jnp.dot(place_ref[0, slot], head_ref[...], preferred_element_type=f32)
        for k in range(4):
            head_stage[pl.ds(slot * 4 + k, devices, stride=16), :] = rows[:, k * 128 : (k + 1) * 128]

    def pack(n, unused):
        block = head_stage[pl.ds(n * 128, 128), :].astype(bf16)
        for k in range(8):
            head_out[n * 8 + k] = block[k * 16 : (k + 1) * 16]
        return unused

    lax.fori_loop(0, devices // 8, pack, 0)
    spread(head_out, head_in, head_send, head_recv, head_local, me)
    route(expert_ref, route_ref, place_ref, mix_ref)

    loads[0].wait()
    squares = jnp.zeros((tokens, 1), f32)
    for n in range(width // 512):
        at = pl.ds(n * 512, 512)
        branch = jnp.dot(head_ref[...], ow_ref[:, at], preferred_element_type=f32)
        stream = (residual_ref[:, at].astype(f32) + branch).astype(bf16).astype(f32)
        stream_ref[:, at] = stream
        squares = squares + jnp.sum(stream * stream, axis=1, keepdims=True)
    inverse = lax.rsqrt(squares / width + EPSILON)
    for n in range(width // 512):
        at = pl.ds(n * 512, 512)
        x_ref[:, at] = (stream_ref[:, at] * inverse * gain_ref[:, at]).astype(bf16)

    collect(place_ref, 1, x_ref, stage_ref, outgoing)
    spread(outgoing, incoming, row_send, row_recv, row_local, me)

    def stage_to(target, side):
        def one(n, unused):
            block = stage_ref[pl.ds(n * 384, 384), :].astype(bf16)
            for k in range(8):
                target[side, n * 8 + k] = block[k * 48 : (k + 1) * 48]
            return unused

        lax.fori_loop(0, devices // 8, one, 0)

    def stage_from(source):
        def one(n, unused):
            for k in range(8):
                at = n * 384 + k * 48
                stage_ref[pl.ds(at, 48), :] = source(n * 8 + k).astype(f32)
            return unused

        lax.fori_loop(0, devices // 8, one, 0)

    def exchange(source, target, send, receive, side):
        spread(source.at[side], target.at[side], send.at[side], receive.at[side], local_sem, me)
        spread_own(source.at[side], target.at[side], local_sem, me)

    def wait_all(buffer, sem, side):
        everyone = buffer.at[side, pl.ds(0, devices - 1)]
        pltpu.make_async_copy(everyone, everyone, sem.at[side]).wait()

    for one in loads[1:4]:
        one.wait()
    gate = jnp.dot(x_ref[...], sg_ref[...], preferred_element_type=f32)
    up = jnp.dot(x_ref[...], su_ref[...], preferred_element_type=f32)
    shared = (gate / (1.0 + jnp.exp(-gate)) * up).astype(bf16)
    for n in range(width // 512):
        at = pl.ds(n * 512, 512)
        total_ref[:, at] = stream_ref[:, at] + jnp.dot(
            shared, sd_ref[:, at], preferred_element_type=f32
        )
    for one in loads[4:]:
        one.wait()

    spread_own(head_out, head_in, head_local, me)
    spread_wait(head_in, head_recv)

    def unpack(n, unused):
        for k in range(8):
            head_stage[pl.ds(n * 128 + k * 16, 16), :] = head_in[n * 8 + k].astype(f32)
        return unused

    lax.fori_loop(0, devices // 8, unpack, 0)

    def first_rows():
        stage_from(lambda at: arrived[at])
        for slot in range(slots):
            for k in range(4):
                head_rows[pl.ds(slot * devices, devices), pl.ds(k * 128, 128)] = head_stage[
                    pl.ds(slot * 4 + k, devices, stride=16), :
                ].astype(bf16)
        for slot in range(slots):
            rows = pl.ds(slot * devices, devices)
            squares = jnp.zeros((devices, 1), f32)
            for n in range(width // 512):
                at = pl.ds(n * 512, 512)
                branch = jnp.dot(head_rows[rows, :], ow_ref[:, at], preferred_element_type=f32)
                base = jnp.concatenate(
                    [
                        stage_ref[pl.ds(slot * chunks + n * 4 + k, devices, stride=slots * chunks), :]
                        for k in range(4)
                    ],
                    axis=1,
                )
                stream = (base + branch).astype(bf16)
                rows_ref[rows, at] = stream
                stream = stream.astype(f32)
                squares = squares + jnp.sum(stream * stream, axis=1, keepdims=True)
            inverse = lax.rsqrt(squares / width + EPSILON)
            for n in range(width // 512):
                at = pl.ds(n * 512, 512)
                rows_ref[rows, at] = (rows_ref[rows, at].astype(f32) * inverse * gain_ref[:, at]).astype(bf16)

    def second_rows():
        spread_own(outgoing, incoming, row_local, me)
        spread_wait(incoming, row_recv)
        stage_from(lambda at: incoming[at])
        for slot in range(slots):
            for k in range(chunks):
                rows_ref[pl.ds(slot * devices, devices), pl.ds(k * 128, 128)] = stage_ref[
                    pl.ds(slot * chunks + k, devices, stride=slots * chunks), :
                ].astype(bf16)

    for side in range(2):
        (first_rows, second_rows)[side]()

        def inner(n, unused):
            at = pl.ds(pl.multiple_of(n * 256, 256), 256)
            gate = jnp.dot(rows_ref[...], eg_ref[side, :, at], preferred_element_type=f32)
            up = jnp.dot(rows_ref[...], eu_ref[side, :, at], preferred_element_type=f32)
            hidden_ref[:, at] = (gate / (1.0 + jnp.exp(-gate)) * up).astype(bf16)
            return unused

        lax.fori_loop(0, hidden // 256, inner, 0)

        def outer(n, unused):
            at = pl.ds(pl.multiple_of(n * 256, 256), 256)
            rows = jnp.dot(hidden_ref[...], ed_ref[side, :, at], preferred_element_type=f32)
            for slot in range(slots):
                for k in range(2):
                    stage_ref[pl.ds(slot * chunks + n * 2 + k, devices, stride=slots * chunks), :] = (
                        rows[slot * devices : (slot + 1) * devices, k * 128 : (k + 1) * 128]
                    )
            return unused

        lax.fori_loop(0, width // 256, outer, 0)
        stage_to(result, side)
        exchange(result, returned, back_send, back_recv, side)

    for side in range(2):
        wait_all(returned, back_recv, side)
        stage_from(lambda at: returned[side, at])
        for k in range(chunks):
            at = pl.ds(k * 128, 128)
            total = total_ref[:, at]
            for slot in range(slots):
                rows = stage_ref[pl.ds(slot * chunks + k, devices, stride=slots * chunks), :].astype(bf16)
                for level in range(2):
                    total = total + jnp.dot(
                        mix_ref[level, side, slot], rows, preferred_element_type=f32
                    )
            total_ref[:, at] = total
    final_ref[...] = total_ref[...].astype(bf16)
    spread_wait(head_out, head_send)
    spread_wait(outgoing, row_send)
    for side in range(2):
        wait_all(result, back_send, side)


def mixture(
    heads, arrived, residual, out_weight, norm_gain, shared_gate, shared_up, shared_down,
    expert_gate, expert_up, expert_down, routed_experts, route_weights,
):
    tokens, width = residual.shape
    hidden = shared_gate.shape[1]
    bf16, f32 = jnp.bfloat16, jnp.float32
    vmem, anywhere = pl.BlockSpec(memory_space=pltpu.VMEM), pl.BlockSpec(memory_space=pl.ANY)
    blocks = (2, 128, 48, 128)
    return pl.pallas_call(
        mixture_kernel,
        out_shape=jax.ShapeDtypeStruct((tokens, width), bf16),
        in_specs=[vmem] * 6 + [anywhere] * 7,
        out_specs=vmem,
        scratch_shapes=[
            pltpu.VMEM(out_weight.shape, bf16),
            pltpu.VMEM(shared_gate.shape, bf16),
            pltpu.VMEM(shared_up.shape, bf16),
            pltpu.VMEM(shared_down.shape, bf16),
            pltpu.VMEM(expert_gate.shape, bf16),
            pltpu.VMEM(expert_up.shape, bf16),
            pltpu.VMEM(expert_down.shape, bf16),
            pltpu.VMEM((tokens, width), f32),
            pltpu.VMEM((tokens, width), bf16),
            pltpu.VMEM((2, 3, 128, tokens), bf16),
            pltpu.VMEM((2, 2, 3, tokens, 128), bf16),
            pltpu.VMEM((128 * 48, 128), f32),
            pltpu.VMEM((128 * 16, 128), f32),
            pltpu.VMEM((128, 16, 128), bf16),
            pltpu.VMEM((128, 16, 128), bf16),
            pltpu.VMEM((384, 512), bf16),
            pltpu.VMEM((384, width), bf16),
            pltpu.VMEM((384, hidden), bf16),
            pltpu.VMEM((128, 48, 128), bf16),
            pltpu.VMEM((128, 48, 128), bf16),
            pltpu.VMEM(blocks, bf16),
            pltpu.VMEM(blocks, bf16),
            pltpu.VMEM((tokens, width), f32),
            pltpu.SemaphoreType.DMA((7,)),
            pltpu.SemaphoreType.DMA,
            pltpu.SemaphoreType.DMA,
            pltpu.SemaphoreType.DMA,
            pltpu.SemaphoreType.DMA,
            pltpu.SemaphoreType.DMA,
            pltpu.SemaphoreType.DMA,
            pltpu.SemaphoreType.DMA((2,)),
            pltpu.SemaphoreType.DMA((2,)),
            pltpu.SemaphoreType.DMA,
        ],
        compiler_params=pltpu.CompilerParams(vmem_limit_bytes=60 << 20, has_side_effects=True),
        name="mixture",
    )(
        heads, arrived, residual, norm_gain.reshape(1, width), routed_experts, route_weights.T,
        out_weight, shared_gate, shared_up, shared_down, expert_gate, expert_up, expert_down,
    )


def body(
    queries,
    key_heads,
    value_heads,
    head_gain,
    residual,
    out_weight,
    norm_gain,
    shared_gate,
    shared_up,
    shared_down,
    expert_gate,
    expert_up,
    expert_down,
    routed_experts,
    route_weights,
):
    experts = routed_experts.T
    heads, arrived = attention(queries, key_heads, value_heads, head_gain, residual, experts)
    return mixture(
        heads,
        arrived,
        residual,
        out_weight,
        norm_gain,
        shared_gate,
        shared_up,
        shared_down,
        expert_gate,
        expert_up,
        expert_down,
        experts,
        route_weights,
    )


def solution(mesh):
    return jax.shard_map(
        body,
        mesh=mesh,
        in_specs=(
            P("sp", "tp"),
            P("sp", "tp"),
            P("sp", "tp"),
            P("tp"),
            P(("sp", "tp"), None),
            P(),
            P(),
            P(),
            P(),
            P(),
            P(("sp", "tp"), None, None),
            P(("sp", "tp"), None, None),
            P(("sp", "tp"), None, None),
            P(("sp", "tp"), None),
            P(("sp", "tp"), None),
        ),
        out_specs=P(("sp", "tp"), None),
        check_vma=False,
    )
```
